512 devices in a mesh: fs: 16 (over y, x), tp: 32 (over z, core).
Axes of the slice: x: 4, y: 4, z: 16, core: 2. Of those that a mesh axis runs over, the one named last changes fastest.
Arguments:
- prompt: bfloat16 [65536, 2048], P(('fs', 'tp')), may hold values from -6 to 6
- norm_gain: float32 [2048], P('tp'), may hold values from 0.1 to 1.9
- gate_master: float32 [32, 2, 512, 2048], P(None, None, 'fs', 'tp'), may hold values from -0.125 to 0.125
- up_master: float32 [32, 2, 512, 2048], P(None, None, 'fs', 'tp'), may hold values from -0.125 to 0.125
- down_master: float32 [32, 2, 512, 2048], P(None, None, 'fs', 'tp'), may hold values from -0.25 to 0.25
- group_pick: int32 [65536, 1], P(('fs', 'tp')), may hold values from 0 to 31; in each aligned block of 128 rows (0 to 127, 128 to 255, ...) at most 8 rows name the same one
- route_weight: bfloat16 [65536, 2], P(('fs', 'tp')), may hold values from 0.099609375 to 1
Outputs:
- gate_serve: bfloat16 [32, 2, 512, 2048], P('tp', None, 'fs')
- up_serve: bfloat16 [32, 2, 512, 2048], P('tp', None, 'fs')
- down_serve: bfloat16 [32, 2, 512, 2048], P('tp', None, 'fs')
- mixed: bfloat16 [65536, 2048], P(('fs', 'tp'))
The draws below stay inside these ranges and needn't reach their ends.
Inputs may be any that keep to these rules, and one draw needn't show every extreme that they name: `group_pick`: in the rows of one device no group is named by more than 8 rows, and in every draw some device's rows name one group exactly 8 times.
All inputs are finite; a program needn't handle non-finite values.
Results may differ from the reference program's by a relative error of at most 0.0081.
Values may be sent and summed in bfloat16 or wider, within the bound.
A program may use at most 64 MiB of HBM per device.

```python
import math
import jax
import jax.numpy as jnp
import numpy as np
from jax import lax

D = 2048
HID = 512
EXP_GRP = 2
TOK_DEV = 128
GROUPS = 32
CAP = 8
TOKENS = 65536


def steps_of(key, shape, shards, smallest, high):
    gain = 1.0
    for position, shards_of in shards:
        heights = jax.random.uniform(jax.random.fold_in(jax.random.fold_in(key, 6), position), (shards_of,), jnp.float32, smallest / len(shards), high / len(shards))
        gain = gain * jnp.repeat(jnp.exp(heights), shape[position] // shards_of).reshape((-1,) + (1,) * (len(shape) - 1 - position))
    return gain


def assign_block(rng, own, number, rows, number_of, top, bound, skew):
    ranking = jax.random.permutation(rng, number_of)
    packed, ordinary = load_shares(number_of, rows * top, bound, skew, True), load_shares(number_of, rows * top, bound, skew, False)
    places = jnp.arange(number_of)

    def named(sizes, rotation):
        used = int((sizes > 0).sum())
        fixed = max(1, used // 4)
        passed = fixed + (places - fixed + rotation * (used - fixed)) % max(1, number_of - fixed)
        return jnp.zeros((number_of,), jnp.int32).at[ranking[jnp.where(places < fixed, places, passed)]].set(jnp.asarray(sizes, jnp.int32))

    sizes = jnp.where(number % 4 == 0, named(packed, number // 4), named(ordinary, number - number // 4 - 1))
    mixed = jax.random.permutation(jax.random.fold_in(own, 3), number_of)
    source_of, taker = mixed[0:number_of // 2 * 2:2], mixed[1:number_of // 2 * 2:2]
    slack = jnp.minimum(sizes[source_of] - 1, bound - sizes[taker]) // 2
    slack = jnp.where((source_of == ranking[0]) | (taker == ranking[0]) | (sizes[taker] == 0), 0, jnp.maximum(slack, 0))
    passed = jax.random.randint(jax.random.fold_in(own, 4), (number_of // 2,), 0, 1 << 20) % (slack + 1)
    sizes = sizes.at[source_of].add(-passed).at[taker].add(passed)
    items = jnp.searchsorted(jnp.cumsum(sizes), jnp.arange(rows * top), side="right").astype(jnp.int32)
    grid = items.reshape(top, rows).T
    grid = grid[jax.random.permutation(jax.random.fold_in(own, 1), rows)]
    rotation = jax.random.randint(jax.random.fold_in(own, 2), (rows, 1), 0, top)
    return jnp.take_along_axis(grid, (jnp.arange(top)[None, :] + rotation) % top, axis=1)


def load_shares(amount, total, reach, skew, full):
    loads = [(1 << 20) // math.isqrt(standing ** skew) + 1 for standing in range(1, amount + 1)]
    largest = reach if full else min(reach, max(-(-total // amount), total * loads[0] // sum(loads)))
    least = 1 if total - largest >= amount - 1 else 0
    given, surplus = [largest] + [least] * (amount - 1), total - largest - least * (amount - 1)
    while surplus > 0:
        movable = [i for i in range(1, amount) if given[i] < largest] or [i for i in range(1, amount) if given[i] < reach]
        whole, budget = sum([loads[i] for i in movable]), surplus
        for i in movable:
            addition = min(reach - given[i], max(1, budget * loads[i] // whole), surplus)
            given[i] = given[i] + addition
            surplus = surplus - addition
    return np.array(given)


def normal_values(own_key, dims, spread, limit, pieces=(), kind=jnp.bfloat16):
    entries = spread * jax.random.normal(own_key, dims, jnp.float32)
    if pieces:
        entries = entries * steps_of(own_key, dims, pieces, -0.22, 0.18)
    return jnp.clip(entries, -limit, limit).astype(kind)


def setup_inputs(seed: int = 0) -> dict:
    splits = jax.random.split(jax.random.key(seed), 8)
    prompt = normal_values(splits[0], (TOKENS, D), 1.0, 6.0, ((0, 512),))
    norm_gain = jnp.clip(1.0 + 0.18 * jax.random.normal(splits[1], (D,), jnp.float32), 0.1, 1.9)
    gate_master = normal_values(splits[2], (GROUPS, EXP_GRP, HID, D), D ** -0.5, 0.125, ((2, 16), (3, 32)), jnp.float32)
    up_master = normal_values(splits[3], (GROUPS, EXP_GRP, HID, D), D ** -0.5, 0.125, ((2, 16), (3, 32)), jnp.float32)
    down_master = normal_values(splits[4], (GROUPS, EXP_GRP, HID, D), HID ** -0.5, 0.25, ((2, 16), (3, 32)), jnp.float32)
    group_pick_keys = jax.random.split(jax.random.fold_in(splits[5], 1), TOKENS // TOK_DEV)
    group_pick_turns = jax.random.permutation(jax.random.fold_in(splits[5], 3), TOKENS // TOK_DEV)
    group_pick = jax.vmap(lambda own, number: assign_block(jax.random.fold_in(splits[5], 2), own, number, TOK_DEV, GROUPS, 1, CAP, 2))(group_pick_keys, group_pick_turns).reshape((TOKENS, 1))
    route_weight = jnp.clip(jnp.exp(math.log(1.0) - 2.306499 * jax.random.uniform(splits[6], (TOKENS, EXP_GRP), jnp.float32) ** steps_of(splits[6], (TOKENS, EXP_GRP), ((0, 512),), -0.2, 0.2)), 0.099609375, 1.0).astype(jnp.bfloat16)
    return dict(prompt=prompt, norm_gain=norm_gain, gate_master=gate_master, up_master=up_master, down_master=down_master, group_pick=group_pick, route_weight=route_weight)


EPS = 1e-06

def reference(prompt, norm_gain, gate_master, up_master, down_master, group_pick, route_weight):
    gate_serve = (gate_master * norm_gain).astype(jnp.bfloat16)
    up_serve = (up_master * norm_gain).astype(jnp.bfloat16)
    down_serve = down_master.astype(jnp.bfloat16)
    values = prompt.astype(jnp.float32)
    normed = (values * lax.rsqrt(lax.optimization_barrier(jnp.mean(values * values, axis=1, keepdims=True)) + EPS)).astype(jnp.bfloat16)
    chosen = group_pick[:, 0].astype(jnp.int32)
    order = jnp.argsort(chosen, stable=True).astype(jnp.int32)
    member = (chosen[:, None] == jnp.arange(GROUPS, dtype=jnp.int32)[None, :]).astype(jnp.int32)
    counts = lax.optimization_barrier(jnp.sum(member, axis=0)).astype(jnp.int32)
    starts = (jnp.cumsum(counts) - counts).astype(jnp.int32)
    row_bound = CAP * (TOKENS // TOK_DEV)
    slot_ids = jnp.arange(row_bound, dtype=jnp.int32)

    def one_group(running, group_index):
        slot_place = jnp.minimum(starts[group_index] + slot_ids, TOKENS - 1).astype(jnp.int32)
        token_ids = order[slot_place].astype(jnp.int32)
        is_valid = slot_ids < counts[group_index]
        group_rows = normed[token_ids].astype(jnp.float32)
        weights = jnp.where(is_valid[:, None], route_weight[token_ids].astype(jnp.float32), 0.0)
        gate_pre = jnp.einsum('sd,ehd->seh', group_rows, gate_serve[group_index].astype(jnp.float32))
        up_pre = jnp.einsum('sd,ehd->seh', group_rows, up_serve[group_index].astype(jnp.float32))
        hidden = (weights[:, :, None] * (jax.nn.silu(gate_pre) * up_pre)).astype(jnp.bfloat16)
        expert_out = jnp.einsum('seh,ehd->sd', hidden.astype(jnp.float32), down_serve[group_index].astype(jnp.float32)).astype(jnp.bfloat16)
        expert_out = jnp.where(is_valid[:, None], expert_out, jnp.zeros_like(expert_out))
        running = running.at[token_ids].add(expert_out)
        return (running, None)
    mixed, _ = lax.scan(one_group, jnp.zeros((TOKENS, D), jnp.bfloat16), jnp.arange(GROUPS, dtype=jnp.int32))
    return (gate_serve, up_serve, down_serve, mixed)
```

```python
import functools

import jax
import jax.numpy as jnp
from jax import lax
from jax.experimental import pallas as pl
from jax.experimental.pallas import tpu as pltpu
from jax.sharding import Mesh
from jax.sharding import PartitionSpec as P

FS = ("y", "x")
TP = ("z", "c")
ALL = ("y", "x", "z", "c")
EPS = 1e-06
MESH = pl.DeviceIdType.MESH
BF = jnp.bfloat16
F32 = jnp.float32

NY, NX, NZ = 4, 4, 16
NT = 2 * NZ
CAP = 8
TOK = 128
D = 2048
LAG1, LAG2, LAG3 = 2, 4, 6
NB = 4


def near(k):
    return ((k + 1) // 2) * (2 * (k % 2) - 1)


def far(i):
    return (8 - (i + 1) // 2) * (2 * (i % 2) - 1)


def body(
    prompt, aux, gain, gate, up, down,
    gs_out, us_out, ds_out, mixed,
    weights, wsend, pxs, pxr, xs, xr, ws, wr, hr, rr, xc, wc, acc, pt,
    px_s, px_r, w_s, w_r, g_s, g_r, x_s, x_r, a_s, a_r, r_s, r_r, o_s,
):
    y, x, z, c = (lax.axis_index(a) for a in ALL)
    me = 2 * z + c
    fs = y * NX + x
    masters = (gate, up, down)

    barrier = pltpu.get_barrier_semaphore()

    @pl.loop(1, NZ)
    def _(k):
        for cc in range(2):
            pl.semaphore_signal(
                barrier, inc=1, device_id={"z": lax.rem(z + k, NZ), "c": cc}, device_id_type=MESH
            )

    for axis, pos, n in (("x", x, NX), ("y", y, NY)):
        for step in (1, n - 1):
            pl.semaphore_signal(
                barrier, inc=1, device_id={axis: lax.rem(pos + step, n)}, device_id_type=MESH
            )
    pl.semaphore_signal(barrier, inc=1, device_id={"c": 1 - c}, device_id_type=MESH)

    gains = gain[...]

    def rounded(a, g):
        value = masters[a][g].reshape(64, 64)
        if a < 2:
            value = value * gains
        return value.astype(BF)

    @pl.loop(0, NZ)
    def _(t):
        for a in range(3):
            pxs[t, a] = rounded(a, 2 * t + 1 - c)

    pl.semaphore_wait(barrier, 2 * (NZ - 1) + 5)
    px = pltpu.make_async_remote_copy(
        src_ref=pxs, dst_ref=pxr, send_sem=px_s, recv_sem=px_r,
        device_id={"c": 1 - c}, device_id_type=MESH,
    )
    px.start()

    values = prompt[...].astype(F32)
    scale = lax.rsqrt(jnp.mean(values * values, axis=1, keepdims=True) + EPS)
    normed = (values * scale).astype(BF)
    rows = lax.broadcasted_iota(jnp.int32, (TOK, TOK), 0)
    cols = lax.broadcasted_iota(jnp.int32, (TOK, TOK), 1)

    def column(row):
        return jnp.sum(jnp.where(rows == cols, row, 0.0), axis=1, keepdims=True)

    pick_row = aux[0:1, :]
    pick_col = column(pick_row)
    same = pick_col == pick_row
    rank_row = jnp.sum(jnp.where(same & (rows < cols), 1.0, 0.0), axis=0, keepdims=True)
    rank_col = jnp.sum(jnp.where(same & (cols < rows), 1.0, 0.0), axis=1, keepdims=True)
    target_row = (pick_row * CAP + rank_row).astype(jnp.int32)
    target_col = (pick_col * CAP + rank_col).astype(jnp.int32)
    slots = lax.broadcasted_iota(jnp.int32, (TOK, NT * CAP), 1)
    pt[...] = (slots == target_col).astype(F32).astype(BF)
    for q in range(4):
        ids = lax.broadcasted_iota(jnp.int32, (64, TOK), 0) + 64 * q
        place = (ids == target_row).astype(F32).astype(BF)
        placed = jnp.dot(place, normed, preferred_element_type=F32)
        xs[8 * q : 8 * q + 8] = placed.reshape(8, CAP, D).astype(BF)
    slot_of = (cols % CAP).astype(F32)
    spread = jnp.where(cols < CAP, column(aux[1:2, :]), column(aux[2:3, :]))
    spread = jnp.where((cols < 2 * CAP) & (rank_col == slot_of), spread, 0.0).astype(BF)
    groups = lax.broadcasted_iota(jnp.int32, (NT, TOK), 0).astype(F32)
    member = (groups == pick_row).astype(F32).astype(BF)
    sent_weights = jnp.dot(member, spread, preferred_element_type=F32)
    for g in range(NT):
        ws[g] = sent_weights[g : g + 1, :]

    px.wait()
    r64 = lax.broadcasted_iota(jnp.int32, (64, 128), 0)
    c64 = lax.broadcasted_iota(jnp.int32, (64, 128), 1)
    own_half = (c64 == r64 + 64 * c).astype(F32).astype(BF)
    other_half = (c64 == r64 + 64 * (1 - c)).astype(F32).astype(BF)
    my_cols = pl.ds(pl.multiple_of(z * 128, 128), 128)

    def weight_copy(t):
        return pltpu.make_async_remote_copy(
            src_ref=wsend.at[t], dst_ref=weights.at[fs, :, :, my_cols],
            send_sem=w_s.at[t], recv_sem=w_r.at[z],
            device_id={"z": t}, device_id_type=MESH,
        )

    def join(t):
        for a in range(3):
            both = jnp.dot(rounded(a, 2 * t + c), own_half, preferred_element_type=F32) + jnp.dot(
                pxr[t, a], other_half, preferred_element_type=F32
            )
            wsend[t, a] = both.astype(BF)

    join(z)
    own_copy = pltpu.make_async_copy(
        wsend.at[z], weights.at[fs, :, :, my_cols], w_r.at[z]
    )
    own_copy.start()

    @pl.loop(1, NZ)
    def _(k):
        t = lax.rem(z + near(k) + NZ, NZ)
        join(t)
        weight_copy(t).start()

    def token_copy(tz, tc):
        t = 2 * tz + tc
        return pltpu.make_async_remote_copy(
            src_ref=xs.at[t], dst_ref=xr.at[me], send_sem=x_s.at[t], recv_sem=x_r.at[me],
            device_id={"z": tz, "c": tc}, device_id_type=MESH,
        )

    def token_weight_copy(tz, tc):
        t = 2 * tz + tc
        return pltpu.make_async_remote_copy(
            src_ref=ws.at[t], dst_ref=wr.at[me], send_sem=a_s.at[t], recv_sem=a_r.at[me],
            device_id={"z": tz, "c": tc}, device_id_type=MESH,
        )

    @pl.loop(0, NZ - 1)
    def _(i):
        tz = lax.rem(z + far(i) + NZ, NZ)
        for tc in range(2):
            token_weight_copy(tz, tc).start()
            token_copy(tz, tc).start()

    token_weight_copy(z, 1 - c).start()
    token_copy(z, 1 - c).start()
    xr[me] = xs[me]
    wr[me] = ws[me]

    def geometry(k):
        along_x = 1 - k % 2
        return along_x, 1 - along_x

    def block(k, da, db):
        ax, ay = geometry(k)
        dx = da * ax + db * ay
        dy = da * ay + db * ax
        return lax.rem(y + dy + NY, NY) * NX + lax.rem(x + dx + NX, NX)

    def piece(k, f):
        col = lax.rem(z + near(k) + NZ, NZ) * 128
        return weights.at[f, :, :, pl.ds(pl.multiple_of(col, 128), 128)]

    def push(k, f, ta, tb):
        ax, ay = geometry(k)
        tx = lax.rem(x + ta * ax + tb * ay + NX, NX)
        ty = lax.rem(y + ta * ay + tb * ax + NY, NY)
        ref = piece(k, f)
        pltpu.make_async_remote_copy(
            src_ref=ref, dst_ref=ref, send_sem=g_s, recv_sem=g_r.at[k, f],
            device_id={"y": ty, "x": tx}, device_id_type=MESH,
        ).start()

    def arrived(k, f):
        ref = piece(k, f)
        pltpu.make_async_copy(ref, ref, g_r.at[k, f]).wait()

    def turn(k):
        return 1 - 2 * ((k // 2) % 2)

    def turn_of(k, da):
        ax, ay = geometry(k)
        a = ax * x + ay * y
        return 1 - 2 * ((a + da + 4 + k // 2) % 2)

    def relay(k, da):
        s = turn_of(k, da)
        f = block(k, da, -s)
        arrived(k, f)
        push(k, f, 0, s)

    def across(k, da):
        f = block(k, da, 0)
        push(k, f, 0, 1)
        push(k, f, 0, -1)

    def stage0(k):
        src = lax.rem(z + near(k) + NZ, NZ)
        pltpu.make_async_copy(piece(k, fs), piece(k, fs), w_r.at[src]).wait()
        push(k, fs, 1, 0)
        push(k, fs, -1, 0)
        across(k, 0)

    def stage1(k):
        s = turn(k)
        f = block(k, -s, 0)
        arrived(k, f)
        push(k, f, s, 0)
        across(k, -s)
        arrived(k, block(k, s, 0))
        across(k, s)
        relay(k, 0)

    def stage2(k):
        arrived(k, block(k, 2, 0))
        across(k, 2)
        relay(k, 1)
        relay(k, -1)

    def stage3(k):
        relay(k, 2)

    @pl.loop(0, NZ + LAG3)
    def _(step):
        pl.when(step < NZ)(lambda: stage0(step))
        pl.when((step >= LAG1) & (step < NZ + LAG1))(lambda: stage1(step - LAG1))
        pl.when((step >= LAG2) & (step < NZ + LAG2))(lambda: stage2(step - LAG2))
        pl.when(step >= LAG3)(lambda: stage3(step - LAG3))

    outs = [
        pltpu.make_async_copy(weights.at[fs, a], out, o_s.at[a])
        for a, out in enumerate((gs_out, us_out, ds_out))
    ]
    for out in outs:
        out.start()

    @pl.loop(0, NZ)
    def _(k):
        for da in (0, 1, -1, 2):
            s = turn_of(k, da)
            arrived(k, block(k, da, s))
            arrived(k, block(k, da, 2))

    lane = lax.broadcasted_iota(jnp.int32, (16, 128), 1)
    row = lax.broadcasted_iota(jnp.int32, (16, 128), 0)
    BZ = NZ // NB
    M = BZ * 16

    @pl.loop(0, NB)
    def _(b):
        @pl.loop(0, BZ)
        def _(j):
            i = b * BZ + j
            sz = lax.rem(z + far(i) + NZ, NZ)
            for sc in range(2):
                t = 2 * sz + sc

                @pl.when((i < NZ - 1) | (c != sc))
                def _():
                    pltpu.make_async_copy(xs.at[t], xr.at[t], x_r.at[t]).wait()
                    pltpu.make_async_copy(ws.at[t], wr.at[t], a_r.at[t]).wait()

            at = pl.ds(pl.multiple_of(j * 16, 16), 16)
            xc[at, :] = xr[pl.ds(2 * sz, 2)].astype(F32).reshape(16, D).astype(BF)
            both = jnp.broadcast_to(wr[pl.ds(2 * sz, 2)], (2, 8, 128)).reshape(16, 128)
            w0 = jnp.sum(jnp.where(lane == row % CAP, both, 0.0), axis=1, keepdims=True)
            w1 = jnp.sum(jnp.where(lane == row % CAP + CAP, both, 0.0), axis=1, keepdims=True)
            wc[at, :] = jnp.where((lane // 32) % 2 == 0, w0, w1)

        acc[...] = jnp.zeros_like(acc)

        @pl.loop(0, 4)
        def _(q):
            part = pl.ds(4 * q, 4)
            nt = (((1,), (1,)), ((), ()))
            xx = xc[...]
            g = lax.dot_general(
                xx, weights[part, 0].reshape(256, D), nt, preferred_element_type=F32
            )
            u = lax.dot_general(
                xx, weights[part, 1].reshape(256, D), nt, preferred_element_type=F32
            )
            w = jnp.concatenate([wc[...], wc[...]], axis=1)
            h = (w * (g / (1.0 + jnp.exp(-g)) * u)).astype(BF)
            acc[...] += jnp.dot(h, weights[part, 2].reshape(256, D), preferred_element_type=F32)

        @pl.loop(0, BZ)
        def _(j):
            i = b * BZ + j
            sz = lax.rem(z + far(i) + NZ, NZ)
            at = pl.ds(pl.multiple_of(j * 16, 16), 16)
            hr[pl.ds(2 * sz, 2)] = acc[at, :].reshape(2, CAP, D).astype(BF)
            for sc in range(2):

                @pl.when((i < NZ - 1) | (c != sc))
                def _():
                    t = 2 * sz + sc
                    pltpu.make_async_remote_copy(
                        src_ref=hr.at[t], dst_ref=rr.at[me], send_sem=r_s.at[t],
                        recv_sem=r_r.at[me], device_id={"z": sz, "c": sc}, device_id_type=MESH,
                    ).start()

    rr[me] = hr[me]

    @pl.loop(1, NT)
    def _(k):
        t = lax.rem(me + k, NT)
        pltpu.make_async_copy(xs.at[t], xr.at[t], x_s.at[t]).wait()
        pltpu.make_async_copy(ws.at[t], wr.at[t], a_s.at[t]).wait()

    @pl.loop(1, NZ)
    def _(k):
        t = lax.rem(z + k, NZ)
        pltpu.make_async_copy(wsend.at[t], wsend.at[t], w_s.at[t]).wait()

    sent = weights.at[pl.ds(0, 15)]
    pltpu.make_async_copy(sent, sent, g_s).wait()
    for out in outs:
        out.wait()

    @pl.loop(1, NT)
    def _(k):
        t = lax.rem(me + k, NT)
        pltpu.make_async_copy(hr.at[t], rr.at[t], r_r.at[t]).wait()
        pltpu.make_async_copy(hr.at[t], rr.at[t], r_s.at[t]).wait()

    for q in range(4):
        cut = slice(512 * q, 512 * q + 512)
        back = rr[:, :, cut].astype(F32).reshape(NT * CAP, 512).astype(BF)
        mixed[:, cut] = jnp.dot(pt[...], back, preferred_element_type=F32).astype(BF)


def per_device(prompt, norm_gain, gate_master, up_master, down_master, group_pick, route_weight):
    aux = jnp.concatenate(
        [
            group_pick.astype(F32).T,
            route_weight.astype(F32).T,
            jnp.zeros((5, TOK), F32),
        ],
        axis=0,
    )
    dma = pltpu.SemaphoreType.DMA
    vmem = pl.BlockSpec(memory_space=pltpu.VMEM)
    hbm = pl.BlockSpec(memory_space=pl.ANY)
    serve = jax.ShapeDtypeStruct((2 * 32, D), BF)
    gs, us, ds, mixed = pl.pallas_call(
        body,
        name="relay",
        out_shape=(serve, serve, serve, jax.ShapeDtypeStruct((TOK, D), BF)),
        in_specs=[vmem] * 6,
        out_specs=(hbm, hbm, hbm, vmem),
        scratch_shapes=[
            pltpu.VMEM((16, 3, 64, D), BF),
            pltpu.VMEM((NZ, 3, 64, 128), BF),
            pltpu.VMEM((NZ, 3, 64, 64), BF),
            pltpu.VMEM((NZ, 3, 64, 64), BF),
            pltpu.VMEM((NT, CAP, D), BF),
            pltpu.VMEM((NT, CAP, D), BF),
            pltpu.VMEM((NT, 1, 128), F32),
            pltpu.VMEM((NT, 1, 128), F32),
            pltpu.VMEM((NT, CAP, D), BF),
            pltpu.VMEM((NT, CAP, D), BF),
            pltpu.VMEM((256 // NB, D), BF),
            pltpu.VMEM((256 // NB, 128), F32),
            pltpu.VMEM((256 // NB, D), F32),
            pltpu.VMEM((TOK, NT * CAP), BF),
            dma, dma,
            dma((NZ,)), dma((NZ,)),
            dma, dma((NZ, 16)),
            dma((NT,)), dma((NT,)),
            dma((NT,)), dma((NT,)),
            dma((NT,)), dma((NT,)),
            dma((3,)),
        ],
        compiler_params=pltpu.CompilerParams(
            collective_id=0, has_side_effects=True, vmem_limit_bytes=56 * 1024 * 1024
        ),
    )(prompt, aux, norm_gain.reshape(1, 64), gate_master, up_master, down_master)
    shape = (1, 2, 32, D)
    return gs.reshape(shape), us.reshape(shape), ds.reshape(shape), mixed


def solution(mesh):
    torus = Mesh(mesh.devices.reshape(NY, NX, NZ, 2), ALL)
    placed = (
        P(ALL, None),
        P(TP),
        P(None, None, FS, TP),
        P(None, None, FS, TP),
        P(None, None, FS, TP),
        P(ALL, None),
        P(ALL, None),
    )
    serve = P(TP, None, FS, None)
    return jax.shard_map(
        per_device,
        mesh=torus,
        in_specs=placed,
        out_specs=(serve, serve, serve, P(ALL, None)),
        check_vma=False,
    )
```

```python
import functools

import jax
import jax.numpy as jnp
from jax import lax
from jax.experimental import pallas as pl
from jax.experimental.pallas import tpu as pltpu
from jax.sharding import Mesh
from jax.sharding import PartitionSpec as P

FS = ("y", "x")
TP = ("z", "c")
ALL = ("y", "x", "z", "c")
EPS = 1e-06
MESH = pl.DeviceIdType.MESH
BF = jnp.bfloat16
F32 = jnp.float32

NY, NX, NZ = 4, 4, 16
NT = 2 * NZ
CAP = 8
TOK = 128
D = 2048
LAG1, LAG2, LAG3 = 2, 4, 6
FIRST = 1
NB = 4


def near(k):
    return ((k + 1) // 2) * (2 * (k % 2) - 1)


def far(i):
    return (8 - (i + 1) // 2) * (2 * (i % 2) - 1)


def body(
    prompt_hbm, pick, route, gain, gate_hbm, up_hbm, down_hbm,
    gs_out, us_out, ds_out, mixed,
    prompt, gate, up, down,
    weights, wsend, pxs, pxr, xs, xr, ws, wr, hr, rr, xc, wc, acc, pt,
    px_s, px_r, w_s, w_r, g_s, g_r, x_s, x_r, a_s, a_r, r_s, r_r, o_s, i_s,
):
    y, x, z, c = (lax.axis_index(a) for a in ALL)
    me = 2 * z + c
    fs = y * NX + x
    masters = (gate, up, down)

    barrier = pltpu.get_barrier_semaphore()

    @pl.loop(0, NZ - 1)
    def _(i):
        tz = lax.rem(z + far(i) + NZ, NZ)
        for cc in range(2):
            pl.semaphore_signal(barrier, inc=1, device_id={"z": tz, "c": cc}, device_id_type=MESH)

    for axis, pos, n in (("x", x, NX), ("y", y, NY)):
        for step in (1, n - 1):
            pl.semaphore_signal(
                barrier, inc=1, device_id={axis: lax.rem(pos + step, n)}, device_id_type=MESH
            )
    pl.semaphore_signal(barrier, inc=1, device_id={"c": 1 - c}, device_id_type=MESH)

    loads = [
        pltpu.make_async_copy(src, dst, i_s.at[n])
        for n, (src, dst) in enumerate(
            ((prompt_hbm, prompt), (gate_hbm, gate), (up_hbm, up), (down_hbm, down))
        )
    ]
    for load in loads:
        load.start()

    gains = gain[...]

    def rounded(a, g):
        value = masters[a][g].reshape(64, 64)
        if a < 2:
            value = value * gains
        return value.astype(BF)

    for load in loads[1:]:
        load.wait()

    @pl.loop(0, NZ)
    def _(t):
        for a in range(3):
            pxs[t, a] = rounded(a, 2 * t + 1 - c)

    loads[0].wait()
    values = prompt[...].astype(F32)
    scale = lax.rsqrt(jnp.mean(values * values, axis=1, keepdims=True) + EPS)
    normed = (values * scale).astype(BF)
    rows = lax.broadcasted_iota(jnp.int32, (TOK, TOK), 0)
    cols = lax.broadcasted_iota(jnp.int32, (TOK, TOK), 1)

    def column(row):
        return jnp.sum(jnp.where(rows == cols, row, 0.0), axis=1, keepdims=True)

    pick_row = pick[...].astype(F32)
    routes = route[...].astype(F32)
    pick_col = column(pick_row)
    same = pick_col == pick_row
    rank_row = jnp.sum(jnp.where(same & (rows < cols), 1.0, 0.0), axis=0, keepdims=True)
    rank_col = jnp.sum(jnp.where(same & (cols < rows), 1.0, 0.0), axis=1, keepdims=True)
    target_row = (pick_row * CAP + rank_row).astype(jnp.int32)
    target_col = (pick_col * CAP + rank_col).astype(jnp.int32)
    slots = lax.broadcasted_iota(jnp.int32, (TOK, NT * CAP), 1)
    pt[...] = (slots == target_col).astype(F32).astype(BF)
    for q in range(4):
        ids = lax.broadcasted_iota(jnp.int32, (64, TOK), 0) + 64 * q
        place = (ids == target_row).astype(F32).astype(BF)
        placed = jnp.dot(place, normed, preferred_element_type=F32)
        xs[8 * q : 8 * q + 8] = placed.reshape(8, CAP, D).astype(BF)
    slot_of = (cols % CAP).astype(F32)
    spread = jnp.where(cols < CAP, column(routes[0:1, :]), column(routes[1:2, :]))
    spread = jnp.where((cols < 2 * CAP) & (rank_col == slot_of), spread, 0.0).astype(BF)
    groups = lax.broadcasted_iota(jnp.int32, (NT, TOK), 0).astype(F32)
    member = (groups == pick_row).astype(F32).astype(BF)
    sent_weights = jnp.dot(member, spread, preferred_element_type=F32)
    for g in range(NT):
        ws[g] = sent_weights[g : g + 1, :]

    pl.semaphore_wait(barrier, 2 * (NZ - 1) + 5)
    px = pltpu.make_async_remote_copy(
        src_ref=pxs, dst_ref=pxr, send_sem=px_s, recv_sem=px_r,
        device_id={"c": 1 - c}, device_id_type=MESH,
    )
    px.start()

    def token_copy(tz, tc):
        t = 2 * tz + tc
        return pltpu.make_async_remote_copy(
            src_ref=xs.at[t], dst_ref=xr.at[me], send_sem=x_s.at[t], recv_sem=x_r.at[me],
            device_id={"z": tz, "c": tc}, device_id_type=MESH,
        )

    def token_weight_copy(tz, tc):
        t = 2 * tz + tc
        return pltpu.make_async_remote_copy(
            src_ref=ws.at[t], dst_ref=wr.at[me], send_sem=a_s.at[t], recv_sem=a_r.at[me],
            device_id={"z": tz, "c": tc}, device_id_type=MESH,
        )

    @pl.loop(0, FIRST)
    def _(i):
        tz = lax.rem(z + far(i) + NZ, NZ)
        for tc in range(2):
            token_weight_copy(tz, tc).start()
            token_copy(tz, tc).start()

    px.wait()
    r64 = lax.broadcasted_iota(jnp.int32, (64, 128), 0)
    c64 = lax.broadcasted_iota(jnp.int32, (64, 128), 1)
    own_half = (c64 == r64 + 64 * c).astype(F32).astype(BF)
    other_half = (c64 == r64 + 64 * (1 - c)).astype(F32).astype(BF)
    my_cols = pl.ds(pl.multiple_of(z * 128, 128), 128)

    def weight_copy(t):
        return pltpu.make_async_remote_copy(
            src_ref=wsend.at[t], dst_ref=weights.at[fs, :, :, my_cols],
            send_sem=w_s.at[t], recv_sem=w_r.at[z],
            device_id={"z": t}, device_id_type=MESH,
        )

    def join(t):
        for a in range(3):
            both = jnp.dot(rounded(a, 2 * t + c), own_half, preferred_element_type=F32) + jnp.dot(
                pxr[t, a], other_half, preferred_element_type=F32
            )
            wsend[t, a] = both.astype(BF)

    join(z)
    own_copy = pltpu.make_async_copy(
        wsend.at[z], weights.at[fs, :, :, my_cols], w_r.at[z]
    )
    own_copy.start()

    @pl.loop(1, NZ)
    def _(k):
        t = lax.rem(z + near(k) + NZ, NZ)
        join(t)
        weight_copy(t).start()

    @pl.loop(FIRST, NZ - 1)
    def _(i):
        tz = lax.rem(z + far(i) + NZ, NZ)
        for tc in range(2):
            token_weight_copy(tz, tc).start()
            token_copy(tz, tc).start()

    token_weight_copy(z, 1 - c).start()
    token_copy(z, 1 - c).start()
    xr[me] = xs[me]
    wr[me] = ws[me]

    def geometry(k):
        along_x = 1 - k % 2
        return along_x, 1 - along_x

    def block(k, da, db):
        ax, ay = geometry(k)
        dx = da * ax + db * ay
        dy = da * ay + db * ax
        return lax.rem(y + dy + NY, NY) * NX + lax.rem(x + dx + NX, NX)

    def piece(k, f):
        col = lax.rem(z + near(k) + NZ, NZ) * 128
        return weights.at[f, :, :, pl.ds(pl.multiple_of(col, 128), 128)]

    def push(k, f, ta, tb):
        ax, ay = geometry(k)
        tx = lax.rem(x + ta * ax + tb * ay + NX, NX)
        ty = lax.rem(y + ta * ay + tb * ax + NY, NY)
        ref = piece(k, f)
        pltpu.make_async_remote_copy(
            src_ref=ref, dst_ref=ref, send_sem=g_s, recv_sem=g_r.at[k, f],
            device_id={"y": ty, "x": tx}, device_id_type=MESH,
        ).start()

    def arrived(k, f):
        ref = piece(k, f)
        pltpu.make_async_copy(ref, ref, g_r.at[k, f]).wait()

    def turn(k):
        return 1 - 2 * ((k // 2) % 2)

    def turn_of(k, da):
        ax, ay = geometry(k)
        a = ax * x + ay * y
        return 1 - 2 * ((a + da + 4 + k // 2) % 2)

    def relay(k, da):
        s = turn_of(k, da)
        f = block(k, da, -s)
        arrived(k, f)
        push(k, f, 0, s)

    def across(k, da):
        f = block(k, da, 0)
        push(k, f, 0, 1)
        push(k, f, 0, -1)

    def stage0(k):
        src = lax.rem(z + near(k) + NZ, NZ)
        pltpu.make_async_copy(piece(k, fs), piece(k, fs), w_r.at[src]).wait()
        push(k, fs, 1, 0)
        push(k, fs, -1, 0)
        across(k, 0)

    def stage1(k):
        s = turn(k)
        f = block(k, -s, 0)
        arrived(k, f)
        push(k, f, s, 0)
        across(k, -s)
        arrived(k, block(k, s, 0))
        across(k, s)
        relay(k, 0)

    def stage2(k):
        arrived(k, block(k, 2, 0))
        across(k, 2)
        relay(k, 1)
        relay(k, -1)

    def stage3(k):
        relay(k, 2)

    @pl.loop(0, NZ + LAG3)
    def _(step):
        pl.when(step < NZ)(lambda: stage0(step))
        pl.when((step >= LAG1) & (step < NZ + LAG1))(lambda: stage1(step - LAG1))
        pl.when((step >= LAG2) & (step < NZ + LAG2))(lambda: stage2(step - LAG2))
        pl.when(step >= LAG3)(lambda: stage3(step - LAG3))

    outs = [
        pltpu.make_async_copy(weights.at[fs, a], out, o_s.at[a])
        for a, out in enumerate((gs_out, us_out, ds_out))
    ]
    for out in outs:
        out.start()

    @pl.loop(0, NZ)
    def _(k):
        for da in (0, 1, -1, 2):
            s = turn_of(k, da)
            arrived(k, block(k, da, s))
            arrived(k, block(k, da, 2))

    lane = lax.broadcasted_iota(jnp.int32, (16, 128), 1)
    row = lax.broadcasted_iota(jnp.int32, (16, 128), 0)
    BZ = NZ // NB
    M = BZ * 16

    @pl.loop(0, NB)
    def _(b):
        @pl.loop(0, BZ)
        def _(j):
            i = b * BZ + j
            sz = lax.rem(z + far(i) + NZ, NZ)
            for sc in range(2):
                t = 2 * sz + sc

                @pl.when((i < NZ - 1) | (c != sc))
                def _():
                    pltpu.make_async_copy(xs.at[t], xr.at[t], x_r.at[t]).wait()
                    pltpu.make_async_copy(ws.at[t], wr.at[t], a_r.at[t]).wait()

            at = pl.ds(pl.multiple_of(j * 16, 16), 16)
            xc[at, :] = xr[pl.ds(2 * sz, 2)].astype(F32).reshape(16, D).astype(BF)
            both = jnp.broadcast_to(wr[pl.ds(2 * sz, 2)], (2, 8, 128)).reshape(16, 128)
            w0 = jnp.sum(jnp.where(lane == row % CAP, both, 0.0), axis=1, keepdims=True)
            w1 = jnp.sum(jnp.where(lane == row % CAP + CAP, both, 0.0), axis=1, keepdims=True)
            wc[at, :] = jnp.where((lane // 32) % 2 == 0, w0, w1)

        acc[...] = jnp.zeros_like(acc)

        @pl.loop(0, 4)
        def _(q):
            part = pl.ds(4 * q, 4)
            nt = (((1,), (1,)), ((), ()))
            xx = xc[...]
            g = lax.dot_general(
                xx, weights[part, 0].reshape(256, D), nt, preferred_element_type=F32
            )
            u = lax.dot_general(
                xx, weights[part, 1].reshape(256, D), nt, preferred_element_type=F32
            )
            w = jnp.concatenate([wc[...], wc[...]], axis=1)
            h = (w * (g / (1.0 + jnp.exp(-g)) * u)).astype(BF)
            acc[...] += jnp.dot(h, weights[part, 2].reshape(256, D), preferred_element_type=F32)

        @pl.loop(0, BZ)
        def _(j):
            i = b * BZ + j
            sz = lax.rem(z + far(i) + NZ, NZ)
            at = pl.ds(pl.multiple_of(j * 16, 16), 16)
            hr[pl.ds(2 * sz, 2)] = acc[at, :].reshape(2, CAP, D).astype(BF)
            for sc in range(2):

                @pl.when((i < NZ - 1) | (c != sc))
                def _():
                    t = 2 * sz + sc
                    pltpu.make_async_remote_copy(
                        src_ref=hr.at[t], dst_ref=rr.at[me], send_sem=r_s.at[t],
                        recv_sem=r_r.at[me], device_id={"z": sz, "c": sc}, device_id_type=MESH,
                    ).start()

    rr[me] = hr[me]

    @pl.loop(1, NT)
    def _(k):
        t = lax.rem(me + k, NT)
        pltpu.make_async_copy(xs.at[t], xr.at[t], x_s.at[t]).wait()
        pltpu.make_async_copy(ws.at[t], wr.at[t], a_s.at[t]).wait()

    @pl.loop(1, NZ)
    def _(k):
        t = lax.rem(z + k, NZ)
        pltpu.make_async_copy(wsend.at[t], wsend.at[t], w_s.at[t]).wait()

    sent = weights.at[pl.ds(0, 15)]
    pltpu.make_async_copy(sent, sent, g_s).wait()
    for out in outs:
        out.wait()

    @pl.loop(1, NT)
    def _(k):
        t = lax.rem(me + k, NT)
        pltpu.make_async_copy(hr.at[t], rr.at[t], r_r.at[t]).wait()
        pltpu.make_async_copy(hr.at[t], rr.at[t], r_s.at[t]).wait()

    for q in range(4):
        cut = slice(512 * q, 512 * q + 512)
        back = rr[:, :, cut].astype(F32).reshape(NT * CAP, 512).astype(BF)
        mixed[:, cut] = jnp.dot(pt[...], back, preferred_element_type=F32).astype(BF)


def written(*refs):
    sems = refs[8]
    copies = [pltpu.make_async_copy(refs[n], refs[4 + n], sems.at[n]) for n in range(4)]
    for copy in copies:
        copy.start()
    for copy in copies:
        copy.wait()


def per_device(prompt, norm_gain, gate_master, up_master, down_master, group_pick, route_weight):
    dma = pltpu.SemaphoreType.DMA
    vmem = pl.BlockSpec(memory_space=pltpu.VMEM)
    hbm = pl.BlockSpec(memory_space=pl.ANY)
    serve = pltpu.VMEM((2 * 32, D), BF)
    gs, us, ds, mixed = pl.pallas_call(
        body,
        name="relay",
        out_shape=(serve, serve, serve, pltpu.VMEM((TOK, D), BF)),
        in_specs=[hbm] + [vmem] * 3 + [hbm] * 3,
        out_specs=(vmem,) * 4,
        scratch_shapes=[
            pltpu.VMEM((TOK, D), BF),
            *[pltpu.VMEM((32, 2, 32, 64), F32)] * 3,
            pltpu.VMEM((16, 3, 64, D), BF),
            pltpu.VMEM((NZ, 3, 64, 128), BF),
            pltpu.VMEM((NZ, 3, 64, 64), BF),
            pltpu.VMEM((NZ, 3, 64, 64), BF),
            pltpu.VMEM((NT, CAP, D), BF),
            pltpu.VMEM((NT, CAP, D), BF),
            pltpu.VMEM((NT, 1, 128), F32),
            pltpu.VMEM((NT, 1, 128), F32),
            pltpu.VMEM((NT, CAP, D), BF),
            pltpu.VMEM((NT, CAP, D), BF),
            pltpu.VMEM((256 // NB, D), BF),
            pltpu.VMEM((256 // NB, 128), F32),
            pltpu.VMEM((256 // NB, D), F32),
            pltpu.VMEM((TOK, NT * CAP), BF),
            dma, dma,
            dma((NZ,)), dma((NZ,)),
            dma, dma((NZ, 16)),
            dma((NT,)), dma((NT,)),
            dma((NT,)), dma((NT,)),
            dma((NT,)), dma((NT,)),
            dma((3,)),
            dma((4,)),
        ],
        compiler_params=pltpu.CompilerParams(
            collective_id=0, has_side_effects=True, vmem_limit_bytes=56 * 1024 * 1024
        ),
    )(prompt, group_pick.T, route_weight.T, norm_gain.reshape(1, 64), gate_master, up_master, down_master)
    gs, us, ds, mixed = pl.pallas_call(
        written,
        name="written",
        out_shape=tuple(jax.ShapeDtypeStruct(a.shape, BF) for a in (gs, us, ds, mixed)),
        in_specs=[vmem] * 4,
        out_specs=(hbm,) * 4,
        scratch_shapes=[dma((4,))],
    )(*(pltpu.with_memory_space_constraint(a, pltpu.VMEM) for a in (gs, us, ds, mixed)))
    shape = (1, 2, 32, D)
    return gs.reshape(shape), us.reshape(shape), ds.reshape(shape), mixed


def solution(mesh):
    torus = Mesh(mesh.devices.reshape(NY, NX, NZ, 2), ALL)
    placed = (
        P(ALL, None),
        P(TP),
        P(None, None, FS, TP),
        P(None, None, FS, TP),
        P(None, None, FS, TP),
        P(ALL, None),
        P(ALL, None),
    )
    serve = P(TP, None, FS, None)
    return jax.shard_map(
        per_device,
        mesh=torus,
        in_specs=placed,
        out_specs=(serve, serve, serve, P(ALL, None)),
        check_vma=False,
    )
```

```python
import functools

import jax
import jax.numpy as jnp
from jax import lax
from jax.experimental import pallas as pl
from jax.experimental.pallas import tpu as pltpu
from jax.sharding import Mesh
from jax.sharding import PartitionSpec as P

FS = ("y", "x")
TP = ("z", "c")
ALL = ("y", "x", "z", "c")
EPS = 1e-06
MESH = pl.DeviceIdType.MESH
BF = jnp.bfloat16
F32 = jnp.float32

NY, NX, NZ = 4, 4, 16
NT = 2 * NZ
CAP = 8
TOK = 128
D = 2048
LAG1, LAG2, LAG3 = 2, 4, 6
EARLY = 3
NB = 4


def near(k):
    return ((k + 1) // 2) * (2 * (k % 2) - 1)


def far(i):
    return (8 - (i + 1) // 2) * (2 * (i % 2) - 1)


def body(
    prompt_hbm, pick, route, gain, gate_hbm, up_hbm, down_hbm,
    gs_out, us_out, ds_out, mixed,
    prompt, gate, up, down,
    weights, wsend, pxs, pxr, xs, xr, ws, wr, hr, rr, xc, wc, acc, pt,
    px_s, px_r, w_s, w_r, g_s, g_r, x_s, x_r, a_s, a_r, r_s, r_r, o_s, i_s, chain, normed,
):
    y, x, z, c = (lax.axis_index(a) for a in ALL)
    me = 2 * z + c
    fs = y * NX + x
    masters = (gate, up, down)

    barrier = pltpu.get_barrier_semaphore()

    for axis, pos, n in (("z", z, NZ), ("x", x, NX), ("y", y, NY)):
        for step in (1, n - 1):
            pl.semaphore_signal(
                barrier, inc=1, device_id={axis: lax.rem(pos + step, n)}, device_id_type=MESH
            )
    pl.semaphore_signal(barrier, inc=1, device_id={"c": 1 - c}, device_id_type=MESH)

    loads = [
        pltpu.make_async_copy(src, dst, i_s.at[n])
        for n, (src, dst) in enumerate(
            ((prompt_hbm, prompt), (gate_hbm, gate), (up_hbm, up), (down_hbm, down))
        )
    ]
    for load in loads:
        load.start()

    gains = gain[...]

    def rounded(a, g):
        value = masters[a][g].reshape(64, 64)
        if a < 2:
            value = value * gains
        return value.astype(BF)

    for load in loads[1:]:
        load.wait()

    @pl.loop(0, NZ)
    def _(t):
        for a in range(3):
            pxs[t, a] = rounded(a, 2 * t + 1 - c)

    pl.semaphore_wait(barrier, 7)

    def tell(j):
        pl.semaphore_signal(
            chain.at[0, j], inc=1, device_id={"z": lax.rem(z + 1, NZ)}, device_id_type=MESH
        )
        pl.semaphore_signal(
            chain.at[1, j], inc=1, device_id={"z": lax.rem(z + NZ - 1, NZ)}, device_id_type=MESH
        )

    def hear(j):
        pl.semaphore_wait(chain.at[0, j], 1)
        pl.semaphore_wait(chain.at[1, j], 1)

    tell(1)
    px = pltpu.make_async_remote_copy(
        src_ref=pxs, dst_ref=pxr, send_sem=px_s, recv_sem=px_r,
        device_id={"c": 1 - c}, device_id_type=MESH,
    )
    px.start()

    loads[0].wait()
    values = prompt[...].astype(F32)
    scale = lax.rsqrt(jnp.mean(values * values, axis=1, keepdims=True) + EPS)
    normed[...] = (values * scale).astype(BF)
    rows = lax.broadcasted_iota(jnp.int32, (TOK, TOK), 0)
    cols = lax.broadcasted_iota(jnp.int32, (TOK, TOK), 1)

    def column(row):
        return jnp.sum(jnp.where(rows == cols, row, 0.0), axis=1, keepdims=True)

    pick_row = pick[...].astype(F32)
    routes = route[...].astype(F32)
    pick_col = column(pick_row)
    same = pick_col == pick_row
    rank_row = jnp.sum(jnp.where(same & (rows < cols), 1.0, 0.0), axis=0, keepdims=True)
    rank_col = jnp.sum(jnp.where(same & (cols < rows), 1.0, 0.0), axis=1, keepdims=True)
    target_row = (pick_row * CAP + rank_row).astype(jnp.int32)
    target_col = (pick_col * CAP + rank_col).astype(jnp.int32)
    slots = lax.broadcasted_iota(jnp.int32, (TOK, NT * CAP), 1)
    pt[...] = (slots == target_col).astype(F32).astype(BF)
    hear(1)
    tell(2)

    r64 = lax.broadcasted_iota(jnp.int32, (64, 128), 0)
    c64 = lax.broadcasted_iota(jnp.int32, (64, 128), 1)
    own_half = (c64 == r64 + 64 * c).astype(F32).astype(BF)
    other_half = (c64 == r64 + 64 * (1 - c)).astype(F32).astype(BF)
    my_cols = pl.ds(pl.multiple_of(z * 128, 128), 128)

    def weight_copy(t):
        return pltpu.make_async_remote_copy(
            src_ref=wsend.at[t], dst_ref=weights.at[fs, :, :, my_cols],
            send_sem=w_s.at[t], recv_sem=w_r.at[z],
            device_id={"z": t}, device_id_type=MESH,
        )

    def join(t, put):
        for a in range(3):
            both = jnp.dot(rounded(a, 2 * t + c), own_half, preferred_element_type=F32) + jnp.dot(
                pxr[t, a], other_half, preferred_element_type=F32
            )
            put(a, both.astype(BF))

    def put_own(a, value):
        weights[fs, a, :, my_cols] = value

    def send_weights(t):
        def put(a, value):
            wsend[t, a] = value

        join(t, put)
        weight_copy(t).start()

    def weights_at(j):
        send_weights(lax.rem(z + j, NZ))
        pl.when(j < NZ // 2)(lambda: send_weights(lax.rem(z + NZ - j, NZ)))

        @pl.when(j <= 6)
        def _():
            hear(j + 2)
            pl.when(j <= 5)(lambda: tell(j + 3))

    def token_copy(tz, tc):
        t = 2 * tz + tc
        return pltpu.make_async_remote_copy(
            src_ref=xs.at[t], dst_ref=xr.at[me], send_sem=x_s.at[t], recv_sem=x_r.at[me],
            device_id={"z": tz, "c": tc}, device_id_type=MESH,
        )

    def token_weight_copy(tz, tc):
        t = 2 * tz + tc
        return pltpu.make_async_remote_copy(
            src_ref=ws.at[t], dst_ref=wr.at[me], send_sem=a_s.at[t], recv_sem=a_r.at[me],
            device_id={"z": tz, "c": tc}, device_id_type=MESH,
        )

    def geometry(k):
        along_x = 1 - k % 2
        return along_x, 1 - along_x

    def block(k, da, db):
        ax, ay = geometry(k)
        dx = da * ax + db * ay
        dy = da * ay + db * ax
        return lax.rem(y + dy + NY, NY) * NX + lax.rem(x + dx + NX, NX)

    def piece(k, f):
        col = lax.rem(z + near(k) + NZ, NZ) * 128
        return weights.at[f, :, :, pl.ds(pl.multiple_of(col, 128), 128)]

    def push(k, f, ta, tb):
        ax, ay = geometry(k)
        tx = lax.rem(x + ta * ax + tb * ay + NX, NX)
        ty = lax.rem(y + ta * ay + tb * ax + NY, NY)
        ref = piece(k, f)
        pltpu.make_async_remote_copy(
            src_ref=ref, dst_ref=ref, send_sem=g_s, recv_sem=g_r.at[k, f],
            device_id={"y": ty, "x": tx}, device_id_type=MESH,
        ).start()

    def arrived(k, f):
        ref = piece(k, f)
        pltpu.make_async_copy(ref, ref, g_r.at[k, f]).wait()

    def turn(k):
        return 1 - 2 * ((k // 2) % 2)

    def turn_of(k, da):
        ax, ay = geometry(k)
        a = ax * x + ay * y
        return 1 - 2 * ((a + da + 4 + k // 2) % 2)

    def relay(k, da):
        s = turn_of(k, da)
        f = block(k, da, -s)
        arrived(k, f)
        push(k, f, 0, s)

    def across(k, da):
        f = block(k, da, 0)
        push(k, f, 0, 1)
        push(k, f, 0, -1)

    def stage0(k):
        src = lax.rem(z + near(k) + NZ, NZ)

        @pl.when(k > 0)
        def _():
            pltpu.make_async_copy(piece(k, fs), piece(k, fs), w_r.at[src]).wait()

        push(k, fs, 1, 0)
        push(k, fs, -1, 0)
        across(k, 0)

    def stage1(k):
        s = turn(k)
        f = block(k, -s, 0)
        arrived(k, f)
        push(k, f, s, 0)
        across(k, -s)
        arrived(k, block(k, s, 0))
        across(k, s)
        relay(k, 0)

    def stage2(k):
        arrived(k, block(k, 2, 0))
        across(k, 2)
        relay(k, 1)
        relay(k, -1)

    def stage3(k):
        relay(k, 2)

    def stages(step):
        pl.when(step < NZ)(lambda: stage0(step))
        pl.when((step >= LAG1) & (step < NZ + LAG1))(lambda: stage1(step - LAG1))
        pl.when((step >= LAG2) & (step < NZ + LAG2))(lambda: stage2(step - LAG2))
        pl.when(step >= LAG3)(lambda: stage3(step - LAG3))

    px.wait()
    join(z, put_own)
    stage0(0)
    hear(2)
    tell(3)

    @pl.loop(1, EARLY + 1)
    def _(j):
        weights_at(j)

    for q in range(4):
        ids = lax.broadcasted_iota(jnp.int32, (64, TOK), 0) + 64 * q
        place = (ids == target_row).astype(F32).astype(BF)
        placed = jnp.dot(place, normed[...], preferred_element_type=F32)
        xs[8 * q : 8 * q + 8] = placed.reshape(8, CAP, D).astype(BF)
    slot_of = (cols % CAP).astype(F32)
    spread = jnp.where(cols < CAP, column(routes[0:1, :]), column(routes[1:2, :]))
    spread = jnp.where((cols < 2 * CAP) & (rank_col == slot_of), spread, 0.0).astype(BF)
    groups = lax.broadcasted_iota(jnp.int32, (NT, TOK), 0).astype(F32)
    member = (groups == pick_row).astype(F32).astype(BF)
    sent_weights = jnp.dot(member, spread, preferred_element_type=F32)
    for g in range(NT):
        ws[g] = sent_weights[g : g + 1, :]

    @pl.loop(1, NZ // 2 - EARLY + 1)
    def _(step):
        weights_at(step + EARLY)
        stages(step)

    @pl.loop(0, NZ - 1)
    def _(i):
        tz = lax.rem(z + far(i) + NZ, NZ)
        for tc in range(2):
            token_weight_copy(tz, tc).start()
            token_copy(tz, tc).start()

    token_weight_copy(z, 1 - c).start()
    token_copy(z, 1 - c).start()
    xr[me] = xs[me]
    wr[me] = ws[me]

    @pl.loop(NZ // 2 - EARLY + 1, NZ + LAG3)
    def _(step):
        stages(step)

    outs = [
        pltpu.make_async_copy(weights.at[fs, a], out, o_s.at[a])
        for a, out in enumerate((gs_out, us_out, ds_out))
    ]
    for out in outs:
        out.start()

    @pl.loop(0, NZ)
    def _(k):
        for da in (0, 1, -1, 2):
            s = turn_of(k, da)
            arrived(k, block(k, da, s))
            arrived(k, block(k, da, 2))

    lane = lax.broadcasted_iota(jnp.int32, (16, 128), 1)
    row = lax.broadcasted_iota(jnp.int32, (16, 128), 0)
    BZ = NZ // NB
    M = BZ * 16

    @pl.loop(0, NB)
    def _(b):
        @pl.loop(0, BZ)
        def _(j):
            i = b * BZ + j
            sz = lax.rem(z + far(i) + NZ, NZ)
            for sc in range(2):
                t = 2 * sz + sc

                @pl.when((i < NZ - 1) | (c != sc))
                def _():
                    pltpu.make_async_copy(xs.at[t], xr.at[t], x_r.at[t]).wait()
                    pltpu.make_async_copy(ws.at[t], wr.at[t], a_r.at[t]).wait()

            at = pl.ds(pl.multiple_of(j * 16, 16), 16)
            xc[at, :] = xr[pl.ds(2 * sz, 2)].astype(F32).reshape(16, D).astype(BF)
            both = jnp.broadcast_to(wr[pl.ds(2 * sz, 2)], (2, 8, 128)).reshape(16, 128)
            w0 = jnp.sum(jnp.where(lane == row % CAP, both, 0.0), axis=1, keepdims=True)
            w1 = jnp.sum(jnp.where(lane == row % CAP + CAP, both, 0.0), axis=1, keepdims=True)
            wc[at, :] = jnp.where((lane // 32) % 2 == 0, w0, w1)

        acc[...] = jnp.zeros_like(acc)

        @pl.loop(0, 4)
        def _(q):
            part = pl.ds(4 * q, 4)
            nt = (((1,), (1,)), ((), ()))
            xx = xc[...]
            g = lax.dot_general(
                xx, weights[part, 0].reshape(256, D), nt, preferred_element_type=F32
            )
            u = lax.dot_general(
                xx, weights[part, 1].reshape(256, D), nt, preferred_element_type=F32
            )
            w = jnp.concatenate([wc[...], wc[...]], axis=1)
            h = (w * (g / (1.0 + jnp.exp(-g)) * u)).astype(BF)
            acc[...] += jnp.dot(h, weights[part, 2].reshape(256, D), preferred_element_type=F32)

        @pl.loop(0, BZ)
        def _(j):
            i = b * BZ + j
            sz = lax.rem(z + far(i) + NZ, NZ)
            at = pl.ds(pl.multiple_of(j * 16, 16), 16)
            hr[pl.ds(2 * sz, 2)] = acc[at, :].reshape(2, CAP, D).astype(BF)
            for sc in range(2):

                @pl.when((i < NZ - 1) | (c != sc))
                def _():
                    t = 2 * sz + sc
                    pltpu.make_async_remote_copy(
                        src_ref=hr.at[t], dst_ref=rr.at[me], send_sem=r_s.at[t],
                        recv_sem=r_r.at[me], device_id={"z": sz, "c": sc}, device_id_type=MESH,
                    ).start()

    rr[me] = hr[me]

    @pl.loop(1, NT)
    def _(k):
        t = lax.rem(me + k, NT)
        pltpu.make_async_copy(xs.at[t], xr.at[t], x_s.at[t]).wait()
        pltpu.make_async_copy(ws.at[t], wr.at[t], a_s.at[t]).wait()

    @pl.loop(1, NZ)
    def _(k):
        t = lax.rem(z + k, NZ)
        pltpu.make_async_copy(wsend.at[t], wsend.at[t], w_s.at[t]).wait()

    sent = weights.at[pl.ds(0, 15)]
    pltpu.make_async_copy(sent, sent, g_s).wait()
    for out in outs:
        out.wait()

    @pl.loop(1, NT)
    def _(k):
        t = lax.rem(me + k, NT)
        pltpu.make_async_copy(hr.at[t], rr.at[t], r_r.at[t]).wait()
        pltpu.make_async_copy(hr.at[t], rr.at[t], r_s.at[t]).wait()

    for q in range(4):
        cut = slice(512 * q, 512 * q + 512)
        back = rr[:, :, cut].astype(F32).reshape(NT * CAP, 512).astype(BF)
        mixed[:, cut] = jnp.dot(pt[...], back, preferred_element_type=F32).astype(BF)


def written(*refs):
    sems = refs[8]
    copies = [pltpu.make_async_copy(refs[n], refs[4 + n], sems.at[n]) for n in range(4)]
    for copy in copies:
        copy.start()
    for copy in copies:
        copy.wait()


def per_device(prompt, norm_gain, gate_master, up_master, down_master, group_pick, route_weight):
    dma = pltpu.SemaphoreType.DMA
    vmem = pl.BlockSpec(memory_space=pltpu.VMEM)
    hbm = pl.BlockSpec(memory_space=pl.ANY)
    serve = pltpu.VMEM((2 * 32, D), BF)
    gs, us, ds, mixed = pl.pallas_call(
        body,
        name="relay",
        out_shape=(serve, serve, serve, pltpu.VMEM((TOK, D), BF)),
        in_specs=[hbm] + [vmem] * 3 + [hbm] * 3,
        out_specs=(vmem,) * 4,
        scratch_shapes=[
            pltpu.VMEM((TOK, D), BF),
            *[pltpu.VMEM((32, 2, 32, 64), F32)] * 3,
            pltpu.VMEM((16, 3, 64, D), BF),
            pltpu.VMEM((NZ, 3, 64, 128), BF),
            pltpu.VMEM((NZ, 3, 64, 64), BF),
            pltpu.VMEM((NZ, 3, 64, 64), BF),
            pltpu.VMEM((NT, CAP, D), BF),
            pltpu.VMEM((NT, CAP, D), BF),
            pltpu.VMEM((NT, 1, 128), F32),
            pltpu.VMEM((NT, 1, 128), F32),
            pltpu.VMEM((NT, CAP, D), BF),
            pltpu.VMEM((NT, CAP, D), BF),
            pltpu.VMEM((256 // NB, D), BF),
            pltpu.VMEM((256 // NB, 128), F32),
            pltpu.VMEM((256 // NB, D), F32),
            pltpu.VMEM((TOK, NT * CAP), BF),
            dma, dma,
            dma((NZ,)), dma((NZ,)),
            dma, dma((NZ, 16)),
            dma((NT,)), dma((NT,)),
            dma((NT,)), dma((NT,)),
            dma((NT,)), dma((NT,)),
            dma((3,)),
            dma((4,)),
            pltpu.SemaphoreType.REGULAR((2, NZ // 2 + 1)),
            pltpu.VMEM((TOK, D), BF),
        ],
        compiler_params=pltpu.CompilerParams(
            collective_id=0, has_side_effects=True, vmem_limit_bytes=56 * 1024 * 1024
        ),
    )(prompt, group_pick.T, route_weight.T, norm_gain.reshape(1, 64), gate_master, up_master, down_master)
    gs, us, ds, mixed = pl.pallas_call(
        written,
        name="written",
        out_shape=tuple(jax.ShapeDtypeStruct(a.shape, BF) for a in (gs, us, ds, mixed)),
        in_specs=[vmem] * 4,
        out_specs=(hbm,) * 4,
        scratch_shapes=[dma((4,))],
    )(*(pltpu.with_memory_space_constraint(a, pltpu.VMEM) for a in (gs, us, ds, mixed)))
    shape = (1, 2, 32, D)
    return gs.reshape(shape), us.reshape(shape), ds.reshape(shape), mixed


def solution(mesh):
    torus = Mesh(mesh.devices.reshape(NY, NX, NZ, 2), ALL)
    placed = (
        P(ALL, None),
        P(TP),
        P(None, None, FS, TP),
        P(None, None, FS, TP),
        P(None, None, FS, TP),
        P(ALL, None),
        P(ALL, None),
    )
    serve = P(TP, None, FS, None)
    return jax.shard_map(
        per_device,
        mesh=torus,
        in_specs=placed,
        out_specs=(serve, serve, serve, P(ALL, None)),
        check_vma=False,
    )
```

```python
import functools

import jax
import jax.numpy as jnp
from jax import lax
from jax.experimental import pallas as pl
from jax.experimental.pallas import tpu as pltpu
from jax.sharding import Mesh
from jax.sharding import PartitionSpec as P

FS = ("y", "x")
TP = ("z", "c")
ALL = ("y", "x", "z", "c")
EPS = 1e-06
MESH = pl.DeviceIdType.MESH
BF = jnp.bfloat16
F32 = jnp.float32

NY, NX, NZ = 4, 4, 16
NT = 2 * NZ
CAP = 8
TOK = 128
D = 2048
LAG1, LAG2, LAG3 = 2, 4, 6
EARLY = 3
NB = 4


def near(k):
    return ((k + 1) // 2) * (2 * (k % 2) - 1)


def far(i):
    return (8 - (i + 1) // 2) * (2 * (i % 2) - 1)


def body(
    prompt_hbm, pick, route, gain, gate_hbm, up_hbm, down_hbm,
    gs_out, us_out, ds_out, mixed,
    prompt, gate, up, down,
    weights, wsend, pxs, pxr, xs, xr, ws, wr, hr, rr, xc, wc, acc, pt,
    px_s, px_r, w_s, w_r, g_s, g_r, g_f, x_s, x_r, a_s, a_r, r_s, r_r, o_s, i_s, chain, normed,
):
    y, x, z, c = (lax.axis_index(a) for a in ALL)
    me = 2 * z + c
    fs = y * NX + x
    masters = (gate, up, down)

    barrier = pltpu.get_barrier_semaphore()

    for axis, pos, n in (("z", z, NZ), ("x", x, NX), ("y", y, NY)):
        for step in (1, n - 1):
            pl.semaphore_signal(
                barrier, inc=1, device_id={axis: lax.rem(pos + step, n)}, device_id_type=MESH
            )
    pl.semaphore_signal(barrier, inc=1, device_id={"c": 1 - c}, device_id_type=MESH)

    loads = [
        pltpu.make_async_copy(src, dst, i_s.at[n])
        for n, (src, dst) in enumerate(
            ((prompt_hbm, prompt), (gate_hbm, gate), (up_hbm, up), (down_hbm, down))
        )
    ]
    for load in loads:
        load.start()

    gains = gain[...]

    def rounded(a, g):
        value = masters[a][g].reshape(64, 64)
        if a < 2:
            value = value * gains
        return value.astype(BF)

    for load in loads[1:]:
        load.wait()

    @pl.loop(0, NZ)
    def _(t):
        for a in range(3):
            pxs[t, a] = rounded(a, 2 * t + 1 - c)

    pl.semaphore_wait(barrier, 7)

    def tell(j):
        pl.semaphore_signal(
            chain.at[0, j], inc=1, device_id={"z": lax.rem(z + 1, NZ)}, device_id_type=MESH
        )
        pl.semaphore_signal(
            chain.at[1, j], inc=1, device_id={"z": lax.rem(z + NZ - 1, NZ)}, device_id_type=MESH
        )

    def hear(j):
        pl.semaphore_wait(chain.at[0, j], 1)
        pl.semaphore_wait(chain.at[1, j], 1)

    tell(1)
    px = pltpu.make_async_remote_copy(
        src_ref=pxs, dst_ref=pxr, send_sem=px_s, recv_sem=px_r,
        device_id={"c": 1 - c}, device_id_type=MESH,
    )
    px.start()

    loads[0].wait()
    values = prompt[...].astype(F32)
    scale = lax.rsqrt(jnp.mean(values * values, axis=1, keepdims=True) + EPS)
    normed[...] = (values * scale).astype(BF)
    rows = lax.broadcasted_iota(jnp.int32, (TOK, TOK), 0)
    cols = lax.broadcasted_iota(jnp.int32, (TOK, TOK), 1)

    def column(row):
        return jnp.sum(jnp.where(rows == cols, row, 0.0), axis=1, keepdims=True)

    pick_row = pick[...].astype(F32)
    routes = route[...].astype(F32)
    pick_col = column(pick_row)
    same = pick_col == pick_row
    rank_row = jnp.sum(jnp.where(same & (rows < cols), 1.0, 0.0), axis=0, keepdims=True)
    rank_col = jnp.sum(jnp.where(same & (cols < rows), 1.0, 0.0), axis=1, keepdims=True)
    target_row = (pick_row * CAP + rank_row).astype(jnp.int32)
    target_col = (pick_col * CAP + rank_col).astype(jnp.int32)
    slots = lax.broadcasted_iota(jnp.int32, (TOK, NT * CAP), 1)
    pt[...] = (slots == target_col).astype(F32).astype(BF)
    hear(1)
    tell(2)

    r64 = lax.broadcasted_iota(jnp.int32, (64, 128), 0)
    c64 = lax.broadcasted_iota(jnp.int32, (64, 128), 1)
    own_half = (c64 == r64 + 64 * c).astype(F32).astype(BF)
    other_half = (c64 == r64 + 64 * (1 - c)).astype(F32).astype(BF)
    my_cols = pl.ds(pl.multiple_of(z * 128, 128), 128)

    def weight_copy(t):
        return pltpu.make_async_remote_copy(
            src_ref=wsend.at[t], dst_ref=weights.at[fs, :, :, my_cols],
            send_sem=w_s, recv_sem=w_r.at[z],
            device_id={"z": t}, device_id_type=MESH,
        )

    def join(t, put):
        for a in range(3):
            both = jnp.dot(rounded(a, 2 * t + c), own_half, preferred_element_type=F32) + jnp.dot(
                pxr[t, a], other_half, preferred_element_type=F32
            )
            put(a, both.astype(BF))

    def put_own(a, value):
        weights[fs, a, :, my_cols] = value

    def send_weights(t):
        def put(a, value):
            wsend[t, a] = value

        join(t, put)
        weight_copy(t).start()

    def weights_at(j):
        send_weights(lax.rem(z + j, NZ))
        pl.when(j < NZ // 2)(lambda: send_weights(lax.rem(z + NZ - j, NZ)))

        @pl.when(j <= 6)
        def _():
            hear(j + 2)
            pl.when(j <= 5)(lambda: tell(j + 3))

    def token_copy(tz, tc, b):
        t = 2 * tz + tc
        return pltpu.make_async_remote_copy(
            src_ref=xs.at[t], dst_ref=xr.at[me], send_sem=x_s, recv_sem=x_r.at[b],
            device_id={"z": tz, "c": tc}, device_id_type=MESH,
        )

    def token_weight_copy(tz, tc):
        t = 2 * tz + tc
        return pltpu.make_async_remote_copy(
            src_ref=ws.at[t], dst_ref=wr.at[me], send_sem=a_s, recv_sem=a_r,
            device_id={"z": tz, "c": tc}, device_id_type=MESH,
        )

    def geometry(k):
        along_x = 1 - k % 2
        return along_x, 1 - along_x

    def block(k, da, db):
        ax, ay = geometry(k)
        dx = da * ax + db * ay
        dy = da * ay + db * ax
        return lax.rem(y + dy + NY, NY) * NX + lax.rem(x + dx + NX, NX)

    def piece(k, f):
        col = lax.rem(z + near(k) + NZ, NZ) * 128
        return weights.at[f, :, :, pl.ds(pl.multiple_of(col, 128), 128)]

    def push(k, f, ta, tb, sem):
        ax, ay = geometry(k)
        tx = lax.rem(x + ta * ax + tb * ay + NX, NX)
        ty = lax.rem(y + ta * ay + tb * ax + NY, NY)
        ref = piece(k, f)
        pltpu.make_async_remote_copy(
            src_ref=ref, dst_ref=ref, send_sem=g_s, recv_sem=sem,
            device_id={"y": ty, "x": tx}, device_id_type=MESH,
        ).start()

    def arrived(k, stage, copies):
        col = lax.rem(z + near(k) + NZ, NZ) * 128
        ref = weights.at[pl.ds(0, copies), :, :, pl.ds(pl.multiple_of(col, 128), 128)]
        pltpu.make_async_copy(ref, ref, g_r.at[k, stage]).wait()

    def turn(k):
        return 1 - 2 * ((k // 2) % 2)

    def turn_of(k, da):
        ax, ay = geometry(k)
        a = ax * x + ay * y
        return 1 - 2 * ((a + da + 4 + k // 2) % 2)

    def relay(k, da):
        s = turn_of(k, da)
        push(k, block(k, da, -s), 0, s, g_f)

    def across(k, da, stage):
        f = block(k, da, 0)
        s = turn_of(k, da)
        push(k, f, 0, s, g_r.at[k, stage])
        push(k, f, 0, -s, g_f)

    def stage0(k):
        src = lax.rem(z + near(k) + NZ, NZ)

        @pl.when(k > 0)
        def _():
            pltpu.make_async_copy(piece(k, fs), piece(k, fs), w_r.at[src]).wait()

        push(k, fs, 1, 0, g_r.at[k, 0])
        push(k, fs, -1, 0, g_r.at[k, 0])
        across(k, 0, 0)

    def stage1(k):
        s = turn(k)
        arrived(k, 0, 3)
        push(k, block(k, -s, 0), s, 0, g_r.at[k, 1])
        across(k, -s, 1)
        across(k, s, 1)
        relay(k, 0)

    def stage2(k):
        arrived(k, 1, 3)
        across(k, 2, 2)
        relay(k, 1)
        relay(k, -1)

    def stage3(k):
        arrived(k, 2, 1)
        relay(k, 2)

    def stages(step):
        pl.when(step < NZ)(lambda: stage0(step))
        pl.when((step >= LAG1) & (step < NZ + LAG1))(lambda: stage1(step - LAG1))
        pl.when((step >= LAG2) & (step < NZ + LAG2))(lambda: stage2(step - LAG2))
        pl.when(step >= LAG3)(lambda: stage3(step - LAG3))

    px.wait()
    join(z, put_own)
    stage0(0)
    hear(2)
    tell(3)

    @pl.loop(1, EARLY + 1)
    def _(j):
        weights_at(j)

    for q in range(4):
        ids = lax.broadcasted_iota(jnp.int32, (64, TOK), 0) + 64 * q
        place = (ids == target_row).astype(F32).astype(BF)
        placed = jnp.dot(place, normed[...], preferred_element_type=F32)
        xs[8 * q : 8 * q + 8] = placed.reshape(8, CAP, D).astype(BF)
    slot_of = (cols % CAP).astype(F32)
    spread = jnp.where(cols < CAP, column(routes[0:1, :]), column(routes[1:2, :]))
    spread = jnp.where((cols < 2 * CAP) & (rank_col == slot_of), spread, 0.0).astype(BF)
    groups = lax.broadcasted_iota(jnp.int32, (NT, TOK), 0).astype(F32)
    member = (groups == pick_row).astype(F32).astype(BF)
    sent_weights = jnp.dot(member, spread, preferred_element_type=F32)
    for g in range(NT):
        ws[g] = sent_weights[g : g + 1, :]

    @pl.loop(1, NZ // 2 - EARLY + 1)
    def _(step):
        weights_at(step + EARLY)
        stages(step)

    @pl.loop(0, NZ - 1)
    def _(i):
        tz = lax.rem(z + far(i) + NZ, NZ)
        for tc in range(2):
            token_weight_copy(tz, tc).start()

    token_weight_copy(z, 1 - c).start()

    @pl.loop(0, NZ - 1)
    def _(i):
        tz = lax.rem(z + far(i) + NZ, NZ)
        place = jnp.where(i > 0, i + 2 * (i % 2) - 1, 0)
        for tc in range(2):
            token_copy(tz, tc, place // (NZ // NB)).start()

    token_copy(z, 1 - c, NB - 1).start()
    xr[me] = xs[me]
    wr[me] = ws[me]

    @pl.loop(NZ // 2 - EARLY + 1, NZ + LAG3)
    def _(step):
        stages(step)

    outs = [
        pltpu.make_async_copy(weights.at[fs, a], out, o_s.at[a])
        for a, out in enumerate((gs_out, us_out, ds_out))
    ]
    for out in outs:
        out.start()

    last = weights.at[pl.ds(0, 8)]
    pltpu.make_async_copy(last, last, g_f).wait()

    lane = lax.broadcasted_iota(jnp.int32, (16, 128), 1)
    row = lax.broadcasted_iota(jnp.int32, (16, 128), 0)
    BZ = NZ // NB
    M = BZ * 16

    def all_of(src, dst, n, sem):
        return pltpu.make_async_copy(src.at[pl.ds(0, n)], dst.at[pl.ds(0, n)], sem)

    all_of(ws, wr, NT - 1, a_r).wait()

    @pl.loop(0, NB)
    def _(b):
        pl.when(b < NB - 1)(lambda: all_of(xs, xr, 2 * BZ, x_r.at[b]).wait())
        pl.when(b == NB - 1)(lambda: all_of(xs, xr, 2 * BZ - 1, x_r.at[b]).wait())

        @pl.loop(0, BZ)
        def _(j):
            i = b * BZ + j
            sz = lax.rem(z + far(i) + NZ, NZ)
            at = pl.ds(pl.multiple_of(j * 16, 16), 16)
            xc[at, :] = xr[pl.ds(2 * sz, 2)].astype(F32).reshape(16, D).astype(BF)
            both = jnp.broadcast_to(wr[pl.ds(2 * sz, 2)], (2, 8, 128)).reshape(16, 128)
            w0 = jnp.sum(jnp.where(lane == row % CAP, both, 0.0), axis=1, keepdims=True)
            w1 = jnp.sum(jnp.where(lane == row % CAP + CAP, both, 0.0), axis=1, keepdims=True)
            wc[at, :] = jnp.where((lane // 32) % 2 == 0, w0, w1)

        acc[...] = jnp.zeros_like(acc)

        @pl.loop(0, 4)
        def _(q):
            part = pl.ds(4 * q, 4)
            nt = (((1,), (1,)), ((), ()))
            xx = xc[...]
            g = lax.dot_general(
                xx, weights[part, 0].reshape(256, D), nt, preferred_element_type=F32
            )
            u = lax.dot_general(
                xx, weights[part, 1].reshape(256, D), nt, preferred_element_type=F32
            )
            w = jnp.concatenate([wc[...], wc[...]], axis=1)
            h = (w * (g / (1.0 + jnp.exp(-g)) * u)).astype(BF)
            acc[...] += jnp.dot(h, weights[part, 2].reshape(256, D), preferred_element_type=F32)

        @pl.loop(0, BZ)
        def _(j):
            i = b * BZ + j
            sz = lax.rem(z + far(i) + NZ, NZ)
            at = pl.ds(pl.multiple_of(j * 16, 16), 16)
            hr[pl.ds(2 * sz, 2)] = acc[at, :].reshape(2, CAP, D).astype(BF)
            for sc in range(2):

                @pl.when((i < NZ - 1) | (c != sc))
                def _():
                    t = 2 * sz + sc
                    pltpu.make_async_remote_copy(
                        src_ref=hr.at[t], dst_ref=rr.at[me], send_sem=r_s,
                        recv_sem=r_r, device_id={"z": sz, "c": sc}, device_id_type=MESH,
                    ).start()

    rr[me] = hr[me]

    all_of(xs, xr, NT - 1, x_s).wait()
    all_of(ws, wr, NT - 1, a_s).wait()
    all_of(wsend, wsend, NZ - 1, w_s).wait()
    sent = weights.at[pl.ds(0, 15)]
    pltpu.make_async_copy(sent, sent, g_s).wait()
    for out in outs:
        out.wait()

    all_of(hr, rr, NT - 1, r_r).wait()
    all_of(hr, rr, NT - 1, r_s).wait()

    for q in range(4):
        cut = slice(512 * q, 512 * q + 512)
        back = rr[:, :, cut].astype(F32).reshape(NT * CAP, 512).astype(BF)
        mixed[:, cut] = jnp.dot(pt[...], back, preferred_element_type=F32).astype(BF)


def written(*refs):
    sems = refs[8]
    copies = [pltpu.make_async_copy(refs[n], refs[4 + n], sems.at[n]) for n in range(4)]
    for copy in copies:
        copy.start()
    for copy in copies:
        copy.wait()


def per_device(prompt, norm_gain, gate_master, up_master, down_master, group_pick, route_weight):
    dma = pltpu.SemaphoreType.DMA
    vmem = pl.BlockSpec(memory_space=pltpu.VMEM)
    hbm = pl.BlockSpec(memory_space=pl.ANY)
    serve = pltpu.VMEM((2 * 32, D), BF)
    gs, us, ds, mixed = pl.pallas_call(
        body,
        name="relay",
        out_shape=(serve, serve, serve, pltpu.VMEM((TOK, D), BF)),
        in_specs=[hbm] + [vmem] * 3 + [hbm] * 3,
        out_specs=(vmem,) * 4,
        scratch_shapes=[
            pltpu.VMEM((TOK, D), BF),
            *[pltpu.VMEM((32, 2, 32, 64), F32)] * 3,
            pltpu.VMEM((16, 3, 64, D), BF),
            pltpu.VMEM((NZ, 3, 64, 128), BF),
            pltpu.VMEM((NZ, 3, 64, 64), BF),
            pltpu.VMEM((NZ, 3, 64, 64), BF),
            pltpu.VMEM((NT, CAP, D), BF),
            pltpu.VMEM((NT, CAP, D), BF),
            pltpu.VMEM((NT, 1, 128), F32),
            pltpu.VMEM((NT, 1, 128), F32),
            pltpu.VMEM((NT, CAP, D), BF),
            pltpu.VMEM((NT, CAP, D), BF),
            pltpu.VMEM((256 // NB, D), BF),
            pltpu.VMEM((256 // NB, 128), F32),
            pltpu.VMEM((256 // NB, D), F32),
            pltpu.VMEM((TOK, NT * CAP), BF),
            dma, dma,
            dma, dma((NZ,)),
            dma, dma((NZ, 3)), dma,
            dma, dma((NB,)),
            dma, dma,
            dma, dma,
            dma((3,)),
            dma((4,)),
            pltpu.SemaphoreType.REGULAR((2, NZ // 2 + 1)),
            pltpu.VMEM((TOK, D), BF),
        ],
        compiler_params=pltpu.CompilerParams(
            collective_id=0, has_side_effects=True, vmem_limit_bytes=56 * 1024 * 1024
        ),
    )(prompt, group_pick.T, route_weight.T, norm_gain.reshape(1, 64), gate_master, up_master, down_master)
    gs, us, ds, mixed = pl.pallas_call(
        written,
        name="written",
        out_shape=tuple(jax.ShapeDtypeStruct(a.shape, BF) for a in (gs, us, ds, mixed)),
        in_specs=[vmem] * 4,
        out_specs=(hbm,) * 4,
        scratch_shapes=[dma((4,))],
    )(*(pltpu.with_memory_space_constraint(a, pltpu.VMEM) for a in (gs, us, ds, mixed)))
    shape = (1, 2, 32, D)
    return gs.reshape(shape), us.reshape(shape), ds.reshape(shape), mixed


def solution(mesh):
    torus = Mesh(mesh.devices.reshape(NY, NX, NZ, 2), ALL)
    placed = (
        P(ALL, None),
        P(TP),
        P(None, None, FS, TP),
        P(None, None, FS, TP),
        P(None, None, FS, TP),
        P(ALL, None),
        P(ALL, None),
    )
    serve = P(TP, None, FS, None)
    return jax.shard_map(
        per_device,
        mesh=torus,
        in_specs=placed,
        out_specs=(serve, serve, serve, P(ALL, None)),
        check_vma=False,
    )
```

```python
import functools

import jax
import jax.numpy as jnp
from jax import lax
from jax.experimental import pallas as pl
from jax.experimental.pallas import tpu as pltpu
from jax.sharding import Mesh
from jax.sharding import PartitionSpec as P

FS = ("y", "x")
TP = ("z", "c")
ALL = ("y", "x", "z", "c")
EPS = 1e-06
MESH = pl.DeviceIdType.MESH
BF = jnp.bfloat16
F32 = jnp.float32

NY, NX, NZ = 4, 4, 16
NT = 2 * NZ
CAP = 8
TOK = 128
D = 2048
LAG1, LAG2, LAG3 = 3, 6, 9
EARLY = 3
NB = 8


def near(k):
    return ((k + 1) // 2) * (2 * (k % 2) - 1)


def far(i):
    return (8 - (i + 1) // 2) * (2 * (i % 2) - 1)


def body(
    prompt_hbm, pick, route, gain, gate_hbm, up_hbm, down_hbm,
    gs_out, us_out, ds_out, mixed,
    prompt, gate, up, down,
    weights, wsend, pxs, pxr, xs, xr, ws, wr, hr, rr, xc, wc, acc, pt,
    px_s, px_r, w_s, w_r, g_s, g_r, g_f, x_s, x_r, a_s, a_r, r_s, r_r, o_s, i_s, chain, normed,
):
    y, x, z, c = (lax.axis_index(a) for a in ALL)
    me = 2 * z + c
    fs = y * NX + x
    masters = (gate, up, down)

    barrier = pltpu.get_barrier_semaphore()

    for axis, pos, n in (("z", z, NZ), ("x", x, NX), ("y", y, NY)):
        for step in (1, n - 1):
            pl.semaphore_signal(
                barrier, inc=1, device_id={axis: lax.rem(pos + step, n)}, device_id_type=MESH
            )
    pl.semaphore_signal(barrier, inc=1, device_id={"c": 1 - c}, device_id_type=MESH)

    loads = [
        pltpu.make_async_copy(src, dst, i_s.at[n])
        for n, (src, dst) in enumerate(
            ((gate_hbm, gate), (up_hbm, up), (down_hbm, down), (prompt_hbm, prompt))
        )
    ]
    for load in loads:
        load.start()

    gains = gain[...]

    def rounded(a, g):
        value = masters[a][g].reshape(64, 64)
        if a < 2:
            value = value * gains
        return value.astype(BF)

    for a in range(3):
        loads[a].wait()

        @pl.loop(0, NZ, unroll=4)
        def _(t):
            pxs[t, a] = rounded(a, 2 * t + 1 - c)

    pl.semaphore_wait(barrier, 7)

    def tell(j):
        pl.semaphore_signal(
            chain.at[0, j], inc=1, device_id={"z": lax.rem(z + 1, NZ)}, device_id_type=MESH
        )
        pl.semaphore_signal(
            chain.at[1, j], inc=1, device_id={"z": lax.rem(z + NZ - 1, NZ)}, device_id_type=MESH
        )

    def hear(j):
        pl.semaphore_wait(chain.at[0, j], 1)
        pl.semaphore_wait(chain.at[1, j], 1)

    tell(1)
    px = pltpu.make_async_remote_copy(
        src_ref=pxs, dst_ref=pxr, send_sem=px_s, recv_sem=px_r,
        device_id={"c": 1 - c}, device_id_type=MESH,
    )
    px.start()

    loads[3].wait()
    values = prompt[...].astype(F32)
    scale = lax.rsqrt(jnp.mean(values * values, axis=1, keepdims=True) + EPS)
    normed[...] = (values * scale).astype(BF)
    rows = lax.broadcasted_iota(jnp.int32, (TOK, TOK), 0)
    cols = lax.broadcasted_iota(jnp.int32, (TOK, TOK), 1)

    def column(row):
        return jnp.sum(jnp.where(rows == cols, row, 0.0), axis=1, keepdims=True)

    pick_row = pick[...].astype(F32)
    routes = route[...].astype(F32)
    pick_col = column(pick_row)
    same = pick_col == pick_row
    rank_row = jnp.sum(jnp.where(same & (rows < cols), 1.0, 0.0), axis=0, keepdims=True)
    rank_col = jnp.sum(jnp.where(same & (cols < rows), 1.0, 0.0), axis=1, keepdims=True)
    target_row = (pick_row * CAP + rank_row).astype(jnp.int32)
    target_col = (pick_col * CAP + rank_col).astype(jnp.int32)
    slots = lax.broadcasted_iota(jnp.int32, (TOK, NT * CAP), 1)
    pt[...] = (slots == target_col).astype(F32).astype(BF)
    hear(1)
    tell(2)

    r64 = lax.broadcasted_iota(jnp.int32, (64, 128), 0)
    c64 = lax.broadcasted_iota(jnp.int32, (64, 128), 1)
    own_half = (c64 == r64 + 64 * c).astype(F32).astype(BF)
    other_half = (c64 == r64 + 64 * (1 - c)).astype(F32).astype(BF)
    my_cols = pl.ds(pl.multiple_of(z * 128, 128), 128)

    def weight_copy(t):
        return pltpu.make_async_remote_copy(
            src_ref=wsend.at[t], dst_ref=weights.at[fs, :, :, my_cols],
            send_sem=w_s, recv_sem=w_r.at[z],
            device_id={"z": t}, device_id_type=MESH,
        )

    def join(t, put):
        for a in range(3):
            both = jnp.dot(rounded(a, 2 * t + c), own_half, preferred_element_type=F32) + jnp.dot(
                pxr[t, a], other_half, preferred_element_type=F32
            )
            put(a, both.astype(BF))

    def put_own(a, value):
        weights[fs, a, :, my_cols] = value

    def send_weights(t):
        def put(a, value):
            wsend[t, a] = value

        join(t, put)
        weight_copy(t).start()

    def weights_at(j):
        send_weights(lax.rem(z + j, NZ))
        pl.when(j < NZ // 2)(lambda: send_weights(lax.rem(z + NZ - j, NZ)))

        @pl.when(j <= 6)
        def _():
            hear(j + 2)
            pl.when(j <= 5)(lambda: tell(j + 3))

    def token_copy(tz, tc, b):
        t = 2 * tz + tc
        return pltpu.make_async_remote_copy(
            src_ref=xs.at[t], dst_ref=xr.at[me], send_sem=x_s, recv_sem=x_r.at[b],
            device_id={"z": tz, "c": tc}, device_id_type=MESH,
        )

    def token_weight_copy(tz, tc):
        t = 2 * tz + tc
        return pltpu.make_async_remote_copy(
            src_ref=ws.at[t], dst_ref=wr.at[me], send_sem=a_s, recv_sem=a_r,
            device_id={"z": tz, "c": tc}, device_id_type=MESH,
        )

    def geometry(k):
        along_x = 1 - k % 2
        return along_x, 1 - along_x

    def block(k, da, db):
        ax, ay = geometry(k)
        dx = da * ax + db * ay
        dy = da * ay + db * ax
        return lax.rem(y + dy + NY, NY) * NX + lax.rem(x + dx + NX, NX)

    def piece(k, f):
        col = lax.rem(z + near(k) + NZ, NZ) * 128
        return weights.at[f, :, :, pl.ds(pl.multiple_of(col, 128), 128)]

    def push(k, f, ta, tb, sem):
        ax, ay = geometry(k)
        tx = lax.rem(x + ta * ax + tb * ay + NX, NX)
        ty = lax.rem(y + ta * ay + tb * ax + NY, NY)
        ref = piece(k, f)
        pltpu.make_async_remote_copy(
            src_ref=ref, dst_ref=ref, send_sem=g_s, recv_sem=sem,
            device_id={"y": ty, "x": tx}, device_id_type=MESH,
        ).start()

    def arrived(k, stage, copies):
        col = lax.rem(z + near(k) + NZ, NZ) * 128
        ref = weights.at[pl.ds(0, copies), :, :, pl.ds(pl.multiple_of(col, 128), 128)]
        pltpu.make_async_copy(ref, ref, g_r.at[k, stage]).wait()

    def turn(k):
        return 1 - 2 * ((k // 2) % 2)

    def turn_of(k, da):
        ax, ay = geometry(k)
        a = ax * x + ay * y
        return 1 - 2 * ((a + da + 4 + k // 2) % 2)

    def relay(k, da):
        s = turn_of(k, da)
        push(k, block(k, da, -s), 0, s, g_f)

    def across(k, da, stage):
        f = block(k, da, 0)
        s = turn_of(k, da)
        push(k, f, 0, s, g_r.at[k, stage])
        push(k, f, 0, -s, g_f)

    def stage0(k):
        src = lax.rem(z + near(k) + NZ, NZ)

        @pl.when(k > 0)
        def _():
            pltpu.make_async_copy(piece(k, fs), piece(k, fs), w_r.at[src]).wait()

        push(k, fs, 1, 0, g_r.at[k, 0])
        push(k, fs, -1, 0, g_r.at[k, 0])
        across(k, 0, 0)

    def stage1(k):
        s = turn(k)
        arrived(k, 0, 3)
        push(k, block(k, -s, 0), s, 0, g_r.at[k, 1])
        across(k, -s, 1)
        across(k, s, 1)
        relay(k, 0)

    def stage2(k):
        arrived(k, 1, 3)
        across(k, 2, 2)
        relay(k, 1)
        relay(k, -1)

    def stage3(k):
        arrived(k, 2, 1)
        relay(k, 2)

    def stages(step):
        pl.when(step < NZ)(lambda: stage0(step))
        pl.when((step >= LAG1) & (step < NZ + LAG1))(lambda: stage1(step - LAG1))
        pl.when((step >= LAG2) & (step < NZ + LAG2))(lambda: stage2(step - LAG2))
        pl.when(step >= LAG3)(lambda: stage3(step - LAG3))

    px.wait()
    join(z, put_own)
    stage0(0)
    hear(2)
    tell(3)

    @pl.loop(1, EARLY + 1)
    def _(j):
        weights_at(j)

    for q in range(4):
        ids = lax.broadcasted_iota(jnp.int32, (64, TOK), 0) + 64 * q
        place = (ids == target_row).astype(F32).astype(BF)
        placed = jnp.dot(place, normed[...], preferred_element_type=F32)
        xs[8 * q : 8 * q + 8] = placed.reshape(8, CAP, D).astype(BF)
    slot_of = (cols % CAP).astype(F32)
    spread = jnp.where(cols < CAP, column(routes[0:1, :]), column(routes[1:2, :]))
    spread = jnp.where((cols < 2 * CAP) & (rank_col == slot_of), spread, 0.0).astype(BF)
    groups = lax.broadcasted_iota(jnp.int32, (NT, TOK), 0).astype(F32)
    member = (groups == pick_row).astype(F32).astype(BF)
    sent_weights = jnp.dot(member, spread, preferred_element_type=F32)
    for g in range(NT):
        ws[g] = sent_weights[g : g + 1, :]

    @pl.loop(1, NZ // 2 - EARLY + 1)
    def _(step):
        weights_at(step + EARLY)
        stages(step)

    @pl.loop(0, NZ - 1)
    def _(i):
        tz = lax.rem(z + far(i) + NZ, NZ)
        for tc in range(2):
            token_weight_copy(tz, tc).start()

    token_weight_copy(z, 1 - c).start()

    @pl.loop(0, NZ - 1)
    def _(i):
        tz = lax.rem(z + far(i) + NZ, NZ)
        place = jnp.where(i > 0, i + 2 * (i % 2) - 1, 0)
        for tc in range(2):
            token_copy(tz, tc, place // (NZ // NB)).start()

    token_copy(z, 1 - c, NB - 1).start()
    xr[me] = xs[me]
    wr[me] = ws[me]

    @pl.loop(NZ // 2 - EARLY + 1, NZ + LAG3)
    def _(step):
        stages(step)

    outs = [
        pltpu.make_async_copy(weights.at[fs, a], out, o_s.at[a])
        for a, out in enumerate((gs_out, us_out, ds_out))
    ]
    for out in outs:
        out.start()

    last = weights.at[pl.ds(0, 8)]
    pltpu.make_async_copy(last, last, g_f).wait()

    lane = lax.broadcasted_iota(jnp.int32, (16, 128), 1)
    row = lax.broadcasted_iota(jnp.int32, (16, 128), 0)
    BZ = NZ // NB
    M = BZ * 16

    def all_of(src, dst, n, sem):
        return pltpu.make_async_copy(src.at[pl.ds(0, n)], dst.at[pl.ds(0, n)], sem)

    all_of(ws, wr, NT - 1, a_r).wait()

    @pl.loop(0, NB)
    def _(b):
        pl.when(b < NB - 1)(lambda: all_of(xs, xr, 2 * BZ, x_r.at[b]).wait())
        pl.when(b == NB - 1)(lambda: all_of(xs, xr, 2 * BZ - 1, x_r.at[b]).wait())

        @pl.loop(0, BZ)
        def _(j):
            i = b * BZ + j
            sz = lax.rem(z + far(i) + NZ, NZ)
            at = pl.ds(pl.multiple_of(j * 16, 16), 16)
            xc[at, :] = xr[pl.ds(2 * sz, 2)].astype(F32).reshape(16, D).astype(BF)
            both = jnp.broadcast_to(wr[pl.ds(2 * sz, 2)], (2, 8, 128)).reshape(16, 128)
            w0 = jnp.sum(jnp.where(lane == row % CAP, both, 0.0), axis=1, keepdims=True)
            w1 = jnp.sum(jnp.where(lane == row % CAP + CAP, both, 0.0), axis=1, keepdims=True)
            wc[at, :] = jnp.where((lane // 32) % 2 == 0, w0, w1)

        acc[...] = jnp.zeros_like(acc)

        @pl.loop(0, 4)
        def _(q):
            part = pl.ds(4 * q, 4)
            nt = (((1,), (1,)), ((), ()))
            xx = xc[...]
            g = lax.dot_general(
                xx, weights[part, 0].reshape(256, D), nt, preferred_element_type=F32
            )
            u = lax.dot_general(
                xx, weights[part, 1].reshape(256, D), nt, preferred_element_type=F32
            )
            w = jnp.concatenate([wc[...], wc[...]], axis=1)
            h = (w * (g / (1.0 + jnp.exp(-g)) * u)).astype(BF)
            acc[...] += jnp.dot(h, weights[part, 2].reshape(256, D), preferred_element_type=F32)

        @pl.loop(0, BZ)
        def _(j):
            i = b * BZ + j
            sz = lax.rem(z + far(i) + NZ, NZ)
            at = pl.ds(pl.multiple_of(j * 16, 16), 16)
            hr[pl.ds(2 * sz, 2)] = acc[at, :].reshape(2, CAP, D).astype(BF)
            for sc in range(2):

                @pl.when((i < NZ - 1) | (c != sc))
                def _():
                    t = 2 * sz + sc
                    pltpu.make_async_remote_copy(
                        src_ref=hr.at[t], dst_ref=rr.at[me], send_sem=r_s,
                        recv_sem=r_r, device_id={"z": sz, "c": sc}, device_id_type=MESH,
                    ).start()

    rr[me] = hr[me]

    all_of(xs, xr, NT - 1, x_s).wait()
    all_of(ws, wr, NT - 1, a_s).wait()
    all_of(wsend, wsend, NZ - 1, w_s).wait()
    sent = weights.at[pl.ds(0, 15)]
    pltpu.make_async_copy(sent, sent, g_s).wait()
    for out in outs:
        out.wait()

    all_of(hr, rr, NT - 1, r_r).wait()
    all_of(hr, rr, NT - 1, r_s).wait()

    for q in range(4):
        cut = slice(512 * q, 512 * q + 512)
        back = rr[:, :, cut].astype(F32).reshape(NT * CAP, 512).astype(BF)
        mixed[:, cut] = jnp.dot(pt[...], back, preferred_element_type=F32).astype(BF)


def written(*refs):
    sems = refs[8]
    copies = [pltpu.make_async_copy(refs[n], refs[4 + n], sems.at[n]) for n in range(4)]
    for copy in copies:
        copy.start()
    for copy in copies:
        copy.wait()


def per_device(prompt, norm_gain, gate_master, up_master, down_master, group_pick, route_weight):
    dma = pltpu.SemaphoreType.DMA
    vmem = pl.BlockSpec(memory_space=pltpu.VMEM)
    hbm = pl.BlockSpec(memory_space=pl.ANY)
    serve = pltpu.VMEM((2 * 32, D), BF)
    gs, us, ds, mixed = pl.pallas_call(
        body,
        name="relay",
        out_shape=(serve, serve, serve, pltpu.VMEM((TOK, D), BF)),
        in_specs=[hbm] + [vmem] * 3 + [hbm] * 3,
        out_specs=(vmem,) * 4,
        scratch_shapes=[
            pltpu.VMEM((TOK, D), BF),
            *[pltpu.VMEM((32, 2, 32, 64), F32)] * 3,
            pltpu.VMEM((16, 3, 64, D), BF),
            pltpu.VMEM((NZ, 3, 64, 128), BF),
            pltpu.VMEM((NZ, 3, 64, 64), BF),
            pltpu.VMEM((NZ, 3, 64, 64), BF),
            pltpu.VMEM((NT, CAP, D), BF),
            pltpu.VMEM((NT, CAP, D), BF),
            pltpu.VMEM((NT, 1, 128), F32),
            pltpu.VMEM((NT, 1, 128), F32),
            pltpu.VMEM((NT, CAP, D), BF),
            pltpu.VMEM((NT, CAP, D), BF),
            pltpu.VMEM((256 // NB, D), BF),
            pltpu.VMEM((256 // NB, 128), F32),
            pltpu.VMEM((256 // NB, D), F32),
            pltpu.VMEM((TOK, NT * CAP), BF),
            dma, dma,
            dma, dma((NZ,)),
            dma, dma((NZ, 3)), dma,
            dma, dma((NB,)),
            dma, dma,
            dma, dma,
            dma((3,)),
            dma((4,)),
            pltpu.SemaphoreType.REGULAR((2, NZ // 2 + 1)),
            pltpu.VMEM((TOK, D), BF),
        ],
        compiler_params=pltpu.CompilerParams(
            collective_id=0, has_side_effects=True, vmem_limit_bytes=56 * 1024 * 1024
        ),
    )(prompt, group_pick.T, route_weight.T, norm_gain.reshape(1, 64), gate_master, up_master, down_master)
    gs, us, ds, mixed = pl.pallas_call(
        written,
        name="written",
        out_shape=tuple(jax.ShapeDtypeStruct(a.shape, BF) for a in (gs, us, ds, mixed)),
        in_specs=[vmem] * 4,
        out_specs=(hbm,) * 4,
        scratch_shapes=[dma((4,))],
    )(*(pltpu.with_memory_space_constraint(a, pltpu.VMEM) for a in (gs, us, ds, mixed)))
    shape = (1, 2, 32, D)
    return gs.reshape(shape), us.reshape(shape), ds.reshape(shape), mixed


def solution(mesh):
    torus = Mesh(mesh.devices.reshape(NY, NX, NZ, 2), ALL)
    placed = (
        P(ALL, None),
        P(TP),
        P(None, None, FS, TP),
        P(None, None, FS, TP),
        P(None, None, FS, TP),
        P(ALL, None),
        P(ALL, None),
    )
    serve = P(TP, None, FS, None)
    return jax.shard_map(
        per_device,
        mesh=torus,
        in_specs=placed,
        out_specs=(serve, serve, serve, P(ALL, None)),
        check_vma=False,
    )
```
